128 devices in a mesh: ep: 128 (over z, y, x, core).
Axes of the slice: x: 4, y: 4, z: 4, core: 2. Of those that a mesh axis runs over, the one named last changes fastest.
Arguments:
- hidden_in: bfloat16 [2048, 2048], P('ep'), may hold values from -6 to 6
- lengths: int32 [2048], P('ep'), may hold values from 1 to 1024
- attn_gain: float32 [2048], replicated, may hold values from 0.1 to 1.9
- query_weight: bfloat16 [2048, 512], replicated, may hold values from -0.125 to 0.125
- key_weight: bfloat16 [2048, 128], replicated, may hold values from -0.125 to 0.125
- value_weight: bfloat16 [2048, 128], replicated, may hold values from -0.125 to 0.125
- score_bias: float32 [8], replicated, may hold values from -7.5 to -3.5
- out_weight: bfloat16 [512, 2048], replicated, may hold values from -0.25 to 0.25
- key_cache: bfloat16 [2048, 1024, 128], P('ep'), may hold values from -6 to 6
- value_cache: bfloat16 [2048, 1024, 128], P('ep'), may hold values from -10 to 10
- ffn_gain: float32 [2048], replicated, may hold values from 0.1 to 1.9
- routes: int32 [2048, 4], P('ep'), may hold values from 0 to 127, all different within a row; in each aligned block of 16 rows (0 to 15, 16 to 31, ...) at most 1 rows name the same one
- route_weights: float32 [2048, 4], P('ep'), may hold values from 0.25 to 1
- expert_gate: bfloat16 [128, 2048, 512], P('ep'), may hold values from -0.125 to 0.125
- expert_up: bfloat16 [128, 2048, 512], P('ep'), may hold values from -0.125 to 0.125
- expert_down: bfloat16 [128, 512, 2048], P('ep'), may hold values from -0.25 to 0.25
- dense_gate: bfloat16 [2048, 2048], P(None, 'ep'), may hold values from -0.125 to 0.125
- dense_up: bfloat16 [2048, 2048], P(None, 'ep'), may hold values from -0.125 to 0.125
- dense_down: bfloat16 [2048, 2048], P(None, 'ep'), may hold values from -0.125 to 0.125
- branch_gate: float32 [2048], replicated, may hold values from -0.125 to 0.125
Outputs:
- hidden_out: bfloat16 [2048, 2048], P('ep')
- new_keys: bfloat16 [2048, 128], P('ep')
- new_values: bfloat16 [2048, 128], P('ep')
The draws below stay inside these ranges and needn't reach their ends.
Inputs may be any that keep to these rules, and one draw needn't show every extreme that they name: `routes`: in each device's 16 rows no expert is named twice.
All inputs are finite; a program needn't handle non-finite values.
Results may differ from the reference program's by a relative error of at most 0.0061.
Values may be sent and summed in bfloat16 or wider, within the bound.
A program may use at most 128 MiB of HBM per device.

```python
import math
import jax
import jax.numpy as jnp
import numpy as np
from jax import lax

D = 2048
HEADS = 8
KV_HEADS = 2
HEAD = 64
LEN = 1024
EFF = 512
TOP = 4
FDENSE = 2048
SEQ_DEV = 16
CAP = 1
BATCH = 2048
EXPERTS = 128


def draw_score_bias(key, part):
    base_key = jax.random.fold_in(key, 11)
    key_slow, key_fast, key_pick = jax.random.split(base_key, 3)
    slow_bias = jax.random.uniform(key_slow, (HEADS,), jnp.float32, -7.5, -6.5)
    fast_bias = jax.random.uniform(key_fast, (HEADS,), jnp.float32, -4.5, -3.5)
    head_order = jax.random.permutation(key_pick, HEADS)
    fast_heads = head_order < HEADS // 2
    return jnp.where(fast_heads, fast_bias, slow_bias)


def draw_value_cache(key, part):
    base_key = jax.random.fold_in(key, 23)
    key_noise, key_block, key_common = jax.random.split(base_key, 3)
    row_width = KV_HEADS * HEAD
    noise_part = jax.random.normal(key_noise, (BATCH, LEN, row_width), jnp.float32)
    block_means = jax.random.normal(key_block, (BATCH, 8, row_width), jnp.float32)
    span_means = jnp.repeat(block_means, LEN // 8, axis=1)
    values_out = noise_part + span_means
    return jnp.clip(values_out, -10.0, 10.0).astype(jnp.bfloat16)


def place_ends(values, key, smallest, high):
    extent = values.shape
    place = [jax.random.randint(jax.random.fold_in(key, axis), (), 0, extent[axis]) for axis in range(len(extent))]
    values = values.at[tuple(place)].set(smallest)
    longest = extent.index(max(extent))
    place[longest] = (place[longest] + 1) % extent[longest]
    return values.at[tuple(place)].set(high)


def block_scale(stream_key, extent, cuts, smallest, largest):
    loudness = 1.0
    for position, blocks in cuts:
        steps = jax.random.uniform(jax.random.fold_in(jax.random.fold_in(stream_key, 6), position), (blocks,), jnp.float32, smallest / len(cuts), largest / len(cuts))
        loudness = loudness * jnp.repeat(jnp.exp(steps), extent[position] // blocks).reshape((-1,) + (1,) * (len(extent) - 1 - position))
    return loudness


def deal_out(key, own, number, rows, number_of, top, most, slope):
    sequence = jax.random.permutation(key, number_of)
    heavy_load, common = shares(number_of, rows * top, most, slope, True), shares(number_of, rows * top, most, slope, False)
    places = jnp.arange(number_of)

    def named(sizes, turn):
        used = int((sizes > 0).sum())
        fixed = max(1, used // 4)
        moved = fixed + (places - fixed + turn * (used - fixed)) % max(1, number_of - fixed)
        return jnp.zeros((number_of,), jnp.int32).at[sequence[jnp.where(places < fixed, places, moved)]].set(jnp.asarray(sizes, jnp.int32))

    sizes = jnp.where(number % 4 == 0, named(heavy_load, number // 4), named(common, number - number // 4 - 1))
    mixed = jax.random.permutation(jax.random.fold_in(own, 3), number_of)
    giver, receiver = mixed[0:number_of // 2 * 2:2], mixed[1:number_of // 2 * 2:2]
    slack = jnp.minimum(sizes[giver] - 1, most - sizes[receiver]) // 2
    slack = jnp.where((giver == sequence[0]) | (receiver == sequence[0]) | (sizes[receiver] == 0), 0, jnp.maximum(slack, 0))
    moved = jax.random.randint(jax.random.fold_in(own, 4), (number_of // 2,), 0, 1 << 20) % (slack + 1)
    sizes = sizes.at[giver].add(-moved).at[receiver].add(moved)
    items = jnp.searchsorted(jnp.cumsum(sizes), jnp.arange(rows * top), side="right").astype(jnp.int32)
    grid = items.reshape(top, rows).T
    grid = grid[jax.random.permutation(jax.random.fold_in(own, 1), rows)]
    turn = jax.random.randint(jax.random.fold_in(own, 2), (rows, 1), 0, top)
    return jnp.take_along_axis(grid, (jnp.arange(top)[None, :] + turn) % top, axis=1)


def shares(count, total, most, skew, full):
    weights = [(1 << 20) // math.isqrt(grade ** skew) + 1 for grade in range(1, count + 1)]
    largest = most if full else min(most, max(-(-total // count), total * weights[0] // sum(weights)))
    least = 1 if total - largest >= count - 1 else 0
    counts, rest = [largest] + [least] * (count - 1), total - largest - least * (count - 1)
    while rest > 0:
        candidates = [i for i in range(1, count) if counts[i] < largest] or [i for i in range(1, count) if counts[i] < most]
        whole, left = sum([weights[i] for i in candidates]), rest
        for i in candidates:
            extra = min(most - counts[i], max(1, left * weights[i] // whole), rest)
            counts[i] = counts[i] + extra
            rest = rest - extra
    return np.array(counts)


def normal_values(own_key, extent, spread, most, cuts=(), kind=jnp.bfloat16):
    drawn = jax.random.normal(own_key, extent, jnp.float32) * spread
    if len(cuts) > 0:
        drawn = block_scale(own_key, extent, cuts, -0.22, 0.18) * drawn
    return jnp.clip(drawn, min=-most, max=most).astype(kind)


def setup_inputs(seed: int = 0) -> dict:
    seeds = jax.random.split(jax.random.key(seed), 21)
    hidden_in = normal_values(seeds[0], (BATCH, D), 1.0, 6.0, ((0, 128),))
    lengths = place_ends(jax.random.randint(seeds[1], (BATCH,), 1, LEN + 1), jax.random.fold_in(seeds[1], 1), 1, LEN).astype(jnp.int32)
    attn_gain = jnp.clip(1.0 + 0.18 * jax.random.normal(seeds[2], (D,), jnp.float32), 0.1, 1.9)
    query_weight = normal_values(seeds[3], (D, HEADS * HEAD), D ** -0.5, 0.125)
    key_weight = normal_values(seeds[4], (D, KV_HEADS * HEAD), D ** -0.5, 0.125)
    value_weight = normal_values(seeds[5], (D, KV_HEADS * HEAD), D ** -0.5, 0.125)
    score_bias = draw_score_bias(jax.random.fold_in(seeds[20], 71), 0)
    out_weight = normal_values(seeds[7], (HEADS * HEAD, D), (HEADS * HEAD) ** -0.5, 0.25)
    key_cache = normal_values(seeds[8], (BATCH, LEN, KV_HEADS * HEAD), 1.0, 6.0, ((0, 128),))
    value_cache = draw_value_cache(jax.random.fold_in(seeds[20], 71), 0)
    ffn_gain = jnp.clip(1.0 + 0.18 * jax.random.normal(seeds[10], (D,), jnp.float32), 0.1, 1.9)
    routes_keys = jax.random.split(jax.random.fold_in(seeds[11], 1), BATCH // SEQ_DEV)
    routes_turns = jax.random.permutation(jax.random.fold_in(seeds[11], 3), BATCH // SEQ_DEV)
    routes = jax.vmap(lambda own, number: deal_out(jax.random.fold_in(seeds[11], 2), own, number, SEQ_DEV, EXPERTS, TOP, CAP, 2))(routes_keys, routes_turns).reshape((BATCH, TOP))
    route_weights = jnp.clip(0.25 + 0.75 * jax.random.uniform(seeds[12], (BATCH, TOP), jnp.float32) ** block_scale(seeds[12], (BATCH, TOP), ((0, 128),), -0.2, 0.2), 0.25, 1.0)
    expert_gate = normal_values(seeds[13], (EXPERTS, D, EFF), D ** -0.5, 0.125, ((0, 128),))
    expert_up = normal_values(seeds[14], (EXPERTS, D, EFF), D ** -0.5, 0.125, ((0, 128),))
    expert_down = normal_values(seeds[15], (EXPERTS, EFF, D), EFF ** -0.5, 0.25, ((0, 128),))
    dense_gate = normal_values(seeds[16], (D, FDENSE), D ** -0.5, 0.125, ((1, 128),))
    dense_up = normal_values(seeds[17], (D, FDENSE), D ** -0.5, 0.125, ((1, 128),))
    dense_down = normal_values(seeds[18], (D, FDENSE), FDENSE ** -0.5, 0.125, ((1, 128),))
    branch_gate = normal_values(seeds[19], (D,), D ** -0.5, 0.125, (), jnp.float32)
    return dict(hidden_in=hidden_in, lengths=lengths, attn_gain=attn_gain, query_weight=query_weight, key_weight=key_weight, value_weight=value_weight, score_bias=score_bias, out_weight=out_weight, key_cache=key_cache, value_cache=value_cache, ffn_gain=ffn_gain, routes=routes, route_weights=route_weights, expert_gate=expert_gate, expert_up=expert_up, expert_down=expert_down, dense_gate=dense_gate, dense_up=dense_up, dense_down=dense_down, branch_gate=branch_gate)


norm_eps = 1e-06

def rms_norm(values_in, gain):
    as_float = values_in.astype(jnp.float32)
    scaled = as_float * lax.rsqrt(lax.optimization_barrier(jnp.mean(as_float * as_float, axis=-1, keepdims=True)) + norm_eps)
    return (scaled * gain).astype(jnp.bfloat16)

def stick_attend(query_blk, key_blk, value_blk, seq_lens, score_bias):
    seq_count = query_blk.shape[0]
    per_group = HEADS // KV_HEADS
    query_f = query_blk.astype(jnp.float32).reshape(seq_count, KV_HEADS, per_group, HEAD)
    key_f = key_blk.astype(jnp.float32).reshape(seq_count, LEN, KV_HEADS, HEAD)
    value_f = value_blk.astype(jnp.float32).reshape(seq_count, LEN, KV_HEADS, HEAD)
    head_bias = score_bias.astype(jnp.float32).reshape(KV_HEADS, per_group)[None, :, :, None]
    scores = jnp.einsum('nkgd,nskd->nkgs', query_f, key_f) * HEAD ** (-0.5) + head_bias
    live_mask = (jnp.arange(LEN, dtype=jnp.int32)[None, :] < seq_lens[:, None])[:, None, None, :]
    log_keep = jnp.where(live_mask, jax.nn.log_sigmoid(-scores), 0.0)
    after_sum = lax.cumsum(log_keep, axis=3, reverse=True) - log_keep
    weights = jnp.where(live_mask, jnp.exp(jax.nn.log_sigmoid(scores) + after_sum), 0.0).astype(jnp.bfloat16)
    weights = lax.optimization_barrier(weights)
    mixed = jnp.einsum('nkgs,nskd->nkgd', weights.astype(jnp.float32), value_f)
    return mixed.astype(jnp.bfloat16).reshape(seq_count, HEADS * HEAD)

def reference(hidden_in, lengths, attn_gain, query_weight, key_weight, value_weight, score_bias, out_weight, key_cache, value_cache, ffn_gain, routes, route_weights, expert_gate, expert_up, expert_down, dense_gate, dense_up, dense_down, branch_gate):
    normed = rms_norm(hidden_in, attn_gain)
    queries = jnp.dot(normed, query_weight, preferred_element_type=jnp.float32).astype(jnp.bfloat16)
    new_keys = jnp.dot(normed, key_weight, preferred_element_type=jnp.float32).astype(jnp.bfloat16)
    new_values = jnp.dot(normed, value_weight, preferred_element_type=jnp.float32).astype(jnp.bfloat16)
    blocks = BATCH // SEQ_DEV

    def attend_block(pieces):
        return stick_attend(pieces[0], pieces[1], pieces[2], pieces[3], score_bias)
    attended = lax.map(attend_block, (queries.reshape(blocks, SEQ_DEV, HEADS * HEAD), key_cache.reshape(blocks, SEQ_DEV, LEN, KV_HEADS * HEAD), value_cache.reshape(blocks, SEQ_DEV, LEN, KV_HEADS * HEAD), lengths.reshape(blocks, SEQ_DEV)))
    attended = attended.reshape(BATCH, HEADS * HEAD)
    middle = hidden_in.astype(jnp.float32) + jnp.dot(attended, out_weight, preferred_element_type=jnp.float32)
    ffn_in = rms_norm(middle, ffn_gain)

    def one_token(pieces):
        token_row, expert_ids, pick_weights = pieces
        row_f = token_row.astype(jnp.float32)
        gate_pre = jnp.einsum('d,kdf->kf', row_f, expert_gate[expert_ids].astype(jnp.float32))
        up_pre = jnp.einsum('d,kdf->kf', row_f, expert_up[expert_ids].astype(jnp.float32))
        hidden_act = lax.optimization_barrier((jax.nn.silu(gate_pre) * up_pre).astype(jnp.bfloat16))
        expert_rows = jnp.einsum('kf,kfd->kd', hidden_act.astype(jnp.float32), expert_down[expert_ids].astype(jnp.float32)).astype(jnp.bfloat16)
        expert_rows = lax.optimization_barrier(expert_rows)
        return lax.optimization_barrier(jnp.sum(pick_weights[:, None] * expert_rows.astype(jnp.float32), axis=0))
    expert_sum = lax.map(one_token, (ffn_in, routes, route_weights))
    gate_pre = jnp.dot(ffn_in, dense_gate, preferred_element_type=jnp.float32)
    up_pre = jnp.dot(ffn_in, dense_up, preferred_element_type=jnp.float32)
    dense_hidden = (jax.nn.silu(gate_pre) * up_pre).astype(jnp.bfloat16)
    dense_out = jnp.dot(dense_hidden, dense_down.T, preferred_element_type=jnp.float32)
    gate_value = jax.nn.sigmoid(jnp.dot(ffn_in.astype(jnp.float32), branch_gate, precision=lax.Precision.HIGHEST))
    hidden_out = (middle + expert_sum + gate_value[:, None] * dense_out).astype(jnp.bfloat16)
    return (hidden_out, new_keys, new_values)
```

```python
import jax
import jax.numpy as jnp
from jax import lax
from jax.experimental import pallas as pl
from jax.experimental.pallas import tpu as pltpu
from jax.sharding import PartitionSpec as P

AXIS = "ep"
DEV = 128
GROUP = 8
RING = 4
SEQ = 16
D = 2048
LEN = 1024
HEAD = 64
HEADS = 8
TOP = 4
EFF = 512
UNITS = 16
CHUNK = 4
EPS = 1e-06
MESH = pl.DeviceIdType.MESH
BF16 = jnp.bfloat16
F32 = jnp.float32


def rms_norm(values, gain):
    scale = lax.rsqrt(jnp.mean(values * values, axis=-1, keepdims=True) + EPS)
    return (values * scale * gain).astype(BF16)


def silu(v):
    return v / (1.0 + jnp.exp(-v))


def nt_dot(a, b):
    return lax.dot_general(a, b, (((1,), (1,)), ((), ())), preferred_element_type=F32)


def dot(a, b):
    return jnp.dot(a, b, preferred_element_type=F32)


def kernel(
    lens,
    bias,
    routes,
    route_weights,
    hid,
    attn_gain,
    ffn_gain,
    branch_gate,
    routes_v,
    qw_h,
    kw_h,
    vw_h,
    ow_h,
    kc_h,
    vc_h,
    eg_h,
    eu_h,
    ed_h,
    dg_h,
    du_h,
    dd_h,
    out,
    new_keys,
    new_values,
    qw,
    kw,
    vw,
    ow,
    kc,
    vc,
    eg,
    eu,
    ed,
    wbuf,
    xg,
    part,
    parts_in,
    tile32,
    send1,
    arr1,
    send2,
    arr2,
    qs,
    os_,
    tri,
    mid_s,
    w_sem,
    k_sem,
    v_sem,
    e_sem,
    d_sem,
    snd,
    rcv,
):
    me = lax.axis_index(AXIS)
    grp = me // GROUP
    mem = lax.rem(me, GROUP)
    zz = grp // RING
    yy = lax.rem(grp, RING)

    def copy(src, dst, sem):
        return pltpu.make_async_copy(src, dst, sem)

    own = [
        copy(dg_h, wbuf.at[zz, yy, pl.ds(0, UNITS)], d_sem.at[0]),
        copy(du_h, wbuf.at[zz, yy, pl.ds(UNITS, UNITS)], d_sem.at[1]),
        copy(dd_h, wbuf.at[zz, yy, pl.ds(2 * UNITS, UNITS)], d_sem.at[2]),
    ]
    proj = [copy(qw_h, qw, w_sem.at[0]), copy(kw_h, kw, w_sem.at[1]), copy(vw_h, vw, w_sem.at[2])]
    outw = [
        copy(
            ow_h.at[pl.ds(h * HEAD, HEAD)],
            ow.at[pl.ds((h % 4) * 2 * HEAD + (h // 4) * HEAD, HEAD)],
            w_sem.at[3 + h],
        )
        for h in range(HEADS)
    ]
    experts = [copy(eg_h.at[0], eg, e_sem.at[0]), copy(eu_h.at[0], eu, e_sem.at[1]), copy(ed_h.at[0], ed, e_sem.at[2])]
    for c in proj + own:
        c.start()

    barrier = pltpu.get_barrier_semaphore()

    @pl.loop(1, DEV)
    def _(d):
        pl.semaphore_signal(barrier, inc=1, device_id=(lax.rem(me + d, DEV),), device_id_type=MESH)

    @pl.loop(0, SEQ)
    def _(b):
        copy(kc_h.at[b], kc.at[b], k_sem.at[b]).start()
        copy(vc_h.at[b], vc.at[b], v_sem.at[b]).start()

    for c in outw + experts:
        c.start()

    row = lax.broadcasted_iota(jnp.int32, (128, 256), 0)
    col = lax.broadcasted_iota(jnp.int32, (128, 256), 1)
    tri[...] = jnp.where((row > col) | (col >= 128), 1.0, 0.0).astype(BF16)

    normed = rms_norm(hid[...].astype(F32), attn_gain[...])
    for c in proj:
        c.wait()
    new_keys[...] = dot(normed, kw[...]).astype(BF16)
    new_values[...] = dot(normed, vw[...]).astype(BF16)
    queries = dot(normed, qw[...]).astype(BF16).astype(F32)
    low = lax.broadcasted_iota(jnp.int32, (SEQ, 128), 1) < HEAD
    for h in range(HEADS):
        piece = queries[:, (h // 2) * 128 : (h // 2 + 1) * 128]
        if (h % 2) != (h // 4):
            piece = pltpu.roll(piece, HEAD, axis=1)
        piece = jnp.where(low, piece, 0.0) if h < 4 else jnp.where(low, 0.0, piece)
        qs[pl.ds(h, SEQ, stride=HEADS), :] = piece

    pl.semaphore_wait(barrier, DEV - 1)
    for c in own:
        c.wait()
    half = D // 2
    left, right = pl.ds(0, half), pl.ds(half, half)

    def device(z, y, member):
        return ((z * RING + y) * GROUP + member,)

    def remote(src, dst, s, to):
        return pltpu.make_async_remote_copy(
            src_ref=src, dst_ref=dst, send_sem=snd.at[s], recv_sem=rcv.at[s], device_id=to, device_id_type=MESH
        )

    for d in (1, 3, 2):
        a = wbuf.at[zz, yy, :, left]
        remote(a, a, 0, device(zz, lax.rem(yy + d, RING), mem)).start()
        b = wbuf.at[zz, yy, :, right]
        remote(b, b, 1, device(lax.rem(zz + d, RING), yy, mem)).start()

    heads = lax.broadcasted_iota(jnp.int32, (HEADS, LEN), 0)
    bias_v = jnp.zeros((HEADS, LEN), F32)
    for h in range(HEADS):
        bias_v = jnp.where(heads == h, bias[h], bias_v)
    pos = lax.broadcasted_iota(jnp.int32, (HEADS, LEN), 1)
    blocks = LEN // 128

    @pl.loop(0, SEQ // CHUNK)
    def _(i):
        logs, keeps, lives = [], [], []
        for j in range(CHUNK):
            b = i * CHUNK + j
            copy(kc_h.at[b], kc.at[b], k_sem.at[b]).wait()
            q = qs[pl.ds(pl.multiple_of(b * HEADS, HEADS), HEADS), :].astype(BF16)
            z = nt_dot(q, kc[b]) * (HEAD**-0.5) + bias_v
            live = pos < lens[b]
            t = jnp.log(1.0 + jnp.exp(-jnp.abs(z)))
            logs.append(jnp.minimum(z, 0.0) - t)
            keeps.append(jnp.where(live, jnp.minimum(-z, 0.0) - t, 0.0))
            lives.append(live)
        keep = jnp.concatenate(
            [keeps[j][:, c * 128 : (c + 1) * 128] for j in range(CHUNK) for c in range(blocks)], axis=0
        )
        hi = keep.astype(BF16)
        rest = keep - hi.astype(F32)
        mid = rest.astype(BF16)
        lo = (rest - mid.astype(F32)).astype(BF16)
        sums = dot(hi, tri[...]) + dot(mid, tri[...]) + dot(lo, tri[...])
        for j in range(CHUNK):
            b = i * CHUNK + j
            beyond = jnp.zeros((HEADS, 128), F32)
            pieces = [None] * blocks
            for c in reversed(range(blocks)):
                at = (j * blocks + c) * HEADS
                after = sums[at : at + HEADS, :128] + beyond
                beyond = beyond + sums[at : at + HEADS, 128:]
                cut = slice(c * 128, (c + 1) * 128)
                pieces[c] = jnp.where(lives[j][:, cut], jnp.exp(logs[j][:, cut] + after), 0.0)
            weights = jnp.concatenate(pieces, axis=1).astype(BF16)
            copy(vc_h.at[b], vc.at[b], v_sem.at[b]).wait()
            os_[pl.ds(pl.multiple_of(b * HEADS, HEADS), HEADS), :] = dot(weights, vc[b])

    for c in outw:
        c.wait()
    attended = []
    for h in range(4):
        first = os_[pl.ds(h, SEQ, stride=HEADS), :]
        second = os_[pl.ds(h + 4, SEQ, stride=HEADS), :]
        attended.append(jnp.where(low, first, second).astype(BF16))
    middle = hid[...].astype(F32) + dot(jnp.concatenate(attended, axis=1), ow[...])
    mid_s[...] = middle
    ffn_in = rms_norm(middle, ffn_gain[...])
    mine = pl.ds(pl.multiple_of(mem * SEQ, SEQ), SEQ)
    xg[mine, :] = ffn_in

    experts_i = lax.broadcasted_iota(jnp.int32, (DEV, SEQ), 0)
    hit = routes_v[0:1, :] == experts_i
    for k in range(1, TOP):
        hit = hit | (routes_v[k : k + 1, :] == experts_i)
    pick = jnp.where(hit, 1.0, 0.0).astype(BF16)

    def to_rows(values, c):
        for j in range(values.shape[1] // 128):
            tile32[pl.ds(c + j, DEV, stride=16), :] = values[:, j * 128 : (j + 1) * 128]

    def pack(dst):
        @pl.loop(0, DEV // 8)
        def _(i):
            for j in range(8):
                r = i * 8 + j
                dst[r] = tile32[pl.ds(pl.multiple_of(r * 16, 16), 16), :].astype(BF16)

    def exchange(src, dst, s):
        @pl.loop(1, DEV)
        def _(d):
            t = lax.rem(me + d, DEV)
            remote(src.at[t], dst.at[me], s, (t,)).start()

    def waited(ref, s):
        copy(ref, ref, snd.at[s]).wait()

    def arrived(ref, s):
        copy(ref, ref, rcv.at[s]).wait()

    for c in range(0, 16, 4):
        to_rows(dot(pick, ffn_in[:, c * 128 : (c + 4) * 128]), c)
    pack(send1)
    exchange(send1, arr1, 2)
    arr1[me] = send1[me]
    for d in (1, 2, 3, 4, 5, 6, 7):
        to = lax.rem(mem + d, GROUP)
        remote(xg.at[mine], xg.at[mine], 3, device(zz, yy, to)).start()

    a_in = wbuf.at[zz, pl.ds(0, RING - 1), :, left]
    b_in = wbuf.at[pl.ds(0, RING - 1), yy, :, right]
    arrived(a_in, 0)
    arrived(b_in, 1)
    for d in (1, 3, 2):
        a = wbuf.at[zz, :, :, left]
        remote(a, a, 4, device(lax.rem(zz + d, RING), yy, mem)).start()
        b = wbuf.at[:, yy, :, right]
        remote(b, b, 5, device(zz, lax.rem(yy + d, RING), mem)).start()

    for c in experts:
        c.wait()
    most = pl.ds(0, DEV - 1)
    arrived(arr1.at[most], 2)

    @pl.loop(0, DEV // 8)
    def _(i):
        for j in range(8):
            r = i * 8 + j
            tile32[pl.ds(pl.multiple_of(r * 16, 16), 16), :] = arr1[r].astype(F32)

    rows = jnp.concatenate([tile32[pl.ds(c, DEV, stride=16), :].astype(BF16) for c in range(16)], axis=1)
    hidden = (silu(dot(rows, eg[...])) * dot(rows, eu[...])).astype(BF16)
    for c in range(0, 16, 4):
        to_rows(dot(hidden, ed[:, c * 128 : (c + 4) * 128]), c)
    pack(send2)
    exchange(send2, arr2, 6)
    arr2[me] = send2[me]

    arrived(xg.at[pl.ds(0, SEQ * (GROUP - 1))], 3)
    arrived(wbuf.at[pl.ds(0, RING - 1), :, :, left], 4)
    arrived(wbuf.at[:, pl.ds(0, RING - 1), :, right], 5)
    tokens = xg[...]

    def share(n):
        return wbuf[:, :, n * UNITS : (n + 1) * UNITS, :].reshape(RING * RING * UNITS, D)

    dense_hidden = (silu(nt_dot(tokens, share(0))) * nt_dot(tokens, share(1))).astype(BF16)
    part[...] = dot(dense_hidden, share(2)).astype(BF16)
    for d in range(1, GROUP):
        to = lax.rem(mem + d, GROUP)
        theirs = pl.ds(pl.multiple_of(to * SEQ, SEQ), SEQ)
        remote(part.at[theirs], parts_in.at[mem], 7, device(zz, yy, to)).start()
    parts_in[mem] = part[mine, :]

    ffn_f = xg[mine, :].astype(F32)
    gate_value = jax.nn.sigmoid(jnp.sum(ffn_f * branch_gate[...], axis=-1, keepdims=True))
    arrived(arr2.at[most], 6)
    for t in range(SEQ):
        total = jnp.zeros((16, 128), F32)
        for k in range(TOP):
            total = total + route_weights[k, t] * arr2[routes[k, t]].astype(F32)
        tile32[pl.ds(t * 16, 16), :] = total
    arrived(parts_in.at[pl.ds(0, GROUP - 1)], 7)
    for c in range(16):
        cut = slice(c * 128, (c + 1) * 128)
        dense = parts_in[0, :, cut].astype(F32)
        for g in range(1, GROUP):
            dense = dense + parts_in[g, :, cut].astype(F32)
        out[:, cut] = (mid_s[:, cut] + tile32[pl.ds(c, SEQ, stride=16), :] + gate_value * dense).astype(BF16)

    waited(a_in, 0)
    waited(b_in, 1)
    waited(send1.at[most], 2)
    waited(xg.at[pl.ds(0, SEQ * (GROUP - 1))], 3)
    waited(wbuf.at[pl.ds(0, RING - 1), :, :, left], 4)
    waited(wbuf.at[:, pl.ds(0, RING - 1), :, right], 5)
    waited(send2.at[most], 6)
    waited(part.at[pl.ds(0, SEQ * (GROUP - 1))], 7)


def per_device(
    hidden_in,
    lengths,
    attn_gain,
    query_weight,
    key_weight,
    value_weight,
    score_bias,
    out_weight,
    key_cache,
    value_cache,
    ffn_gain,
    routes,
    route_weights,
    expert_gate,
    expert_up,
    expert_down,
    dense_gate,
    dense_up,
    dense_down,
    branch_gate,
):
    smem = pl.BlockSpec(memory_space=pltpu.SMEM)
    vmem = pl.BlockSpec(memory_space=pltpu.VMEM)
    hbm = pl.BlockSpec(memory_space=pl.ANY)
    routes_t = routes.T
    dma = pltpu.SemaphoreType.DMA
    return tuple(
        pl.pallas_call(
            kernel,
            name="decode_layer",
            out_shape=(
                jax.ShapeDtypeStruct((SEQ, D), BF16),
                jax.ShapeDtypeStruct((SEQ, 128), BF16),
                jax.ShapeDtypeStruct((SEQ, 128), BF16),
            ),
            in_specs=[smem] * 4 + [vmem] * 5 + [hbm] * 12,
            out_specs=(vmem, vmem, vmem),
            scratch_shapes=[
                pltpu.VMEM((D, HEADS * HEAD), BF16),
                pltpu.VMEM((D, 128), BF16),
                pltpu.VMEM((D, 128), BF16),
                pltpu.VMEM((HEADS * HEAD, D), BF16),
                pltpu.VMEM((SEQ, LEN, 128), BF16),
                pltpu.VMEM((SEQ, LEN, 128), BF16),
                pltpu.VMEM((D, EFF), BF16),
                pltpu.VMEM((D, EFF), BF16),
                pltpu.VMEM((EFF, D), BF16),
                pltpu.VMEM((RING, RING, 3 * UNITS, D), BF16),
                pltpu.VMEM((GROUP * SEQ, D), BF16),
                pltpu.VMEM((GROUP * SEQ, D), BF16),
                pltpu.VMEM((GROUP, SEQ, D), BF16),
                pltpu.VMEM((DEV * 16, 128), F32),
                pltpu.VMEM((DEV, 16, 128), BF16),
                pltpu.VMEM((DEV, 16, 128), BF16),
                pltpu.VMEM((DEV, 16, 128), BF16),
                pltpu.VMEM((DEV, 16, 128), BF16),
                pltpu.VMEM((SEQ * HEADS, 128), F32),
                pltpu.VMEM((SEQ * HEADS, 128), F32),
                pltpu.VMEM((128, 256), BF16),
                pltpu.VMEM((SEQ, D), F32),
                dma((3 + HEADS,)),
                dma((SEQ,)),
                dma((SEQ,)),
                dma((3,)),
                dma((3,)),
                dma((8,)),
                dma((8,)),
            ],
            compiler_params=pltpu.CompilerParams(
                collective_id=0, has_side_effects=True, vmem_limit_bytes=60 * 1024 * 1024
            ),
        )(
            lengths,
            score_bias,
            routes_t,
            route_weights.T,
            hidden_in,
            attn_gain.reshape(1, D),
            ffn_gain.reshape(1, D),
            branch_gate.reshape(1, D),
            routes_t,
            query_weight,
            key_weight,
            value_weight,
            out_weight,
            key_cache,
            value_cache,
            expert_gate,
            expert_up,
            expert_down,
            dense_gate.T,
            dense_up.T,
            dense_down.T,
        )
    )


def solution(mesh):
    return jax.shard_map(
        per_device,
        mesh=mesh,
        in_specs=(
            P("ep", None),
            P("ep"),
            P(),
            P(),
            P(),
            P(),
            P(),
            P(),
            P("ep", None, None),
            P("ep", None, None),
            P(),
            P("ep", None),
            P("ep", None),
            P("ep", None, None),
            P("ep", None, None),
            P("ep", None, None),
            P(None, "ep"),
            P(None, "ep"),
            P(None, "ep"),
            P(),
        ),
        out_specs=(P("ep", None), P("ep", None), P("ep", None)),
        check_vma=False,
    )
```

```python
import jax
import jax.numpy as jnp
from jax import lax
from jax.experimental import pallas as pl
from jax.experimental.pallas import tpu as pltpu
from jax.sharding import PartitionSpec as P

AXIS = "ep"
DEV = 128
GROUP = 8
RING = 4
SEQ = 16
D = 2048
LEN = 1024
HEAD = 64
HEADS = 8
TOP = 4
EFF = 512
UNITS = 16
EPS = 1e-06
MESH = pl.DeviceIdType.MESH
BF16 = jnp.bfloat16
F32 = jnp.float32


def rms_norm(values, gain):
    scale = lax.rsqrt(jnp.mean(values * values, axis=-1, keepdims=True) + EPS)
    return (values * scale * gain).astype(BF16)


def silu(v):
    return v / (1.0 + jnp.exp(-v))


def nt_dot(a, b):
    return lax.dot_general(a, b, (((1,), (1,)), ((), ())), preferred_element_type=F32)


def dot(a, b):
    return jnp.dot(a, b, preferred_element_type=F32)


def kernel(
    lens_h,
    bias_h,
    routes_h,
    route_weights_h,
    hid_h,
    attn_gain_h,
    ffn_gain_h,
    branch_gate_h,
    qw_h,
    kw_h,
    vw_h,
    ow_h,
    kc_h,
    vc_h,
    eg_h,
    eu_h,
    ed_h,
    dg_h,
    du_h,
    dd_h,
    out_h,
    new_keys_h,
    new_values_h,
    lens,
    bias,
    routes,
    route_weights,
    hid,
    attn_gain,
    ffn_gain,
    branch_gate,
    routes_v,
    out,
    new_keys,
    new_values,
    qw,
    kw,
    vw,
    ow,
    kc,
    vc,
    eg,
    eu,
    ed,
    wbuf,
    xg,
    part,
    part2,
    pair_in,
    parts_in,
    tile32,
    send1,
    arr1,
    send2,
    arr2,
    qs,
    os_,
    tri,
    mid_s,
    s_sem,
    o_sem,
    w_sem,
    k_sem,
    v_sem,
    e_sem,
    d_sem,
    snd,
    rcv,
    ready,
):
    me = lax.axis_index(AXIS)
    grp = me // GROUP
    mem = lax.rem(me, GROUP)
    zz = grp // RING
    yy = lax.rem(grp, RING)

    def device(z, y, member):
        return ((z * RING + y) * GROUP + member,)

    in_y = [device(zz, lax.rem(yy + d, RING), mem) for d in (1, 3, 2)]
    in_z = [device(lax.rem(zz + d, RING), yy, mem) for d in (1, 3, 2)]
    xx, core = mem // 2, lax.rem(mem, 2)
    in_x = [device(zz, yy, lax.rem(xx + d, RING) * 2 + core) for d in (1, 3, 2)]
    sibling = device(zz, yy, xx * 2 + 1 - core)
    in_group = [device(zz, yy, lax.rem(mem + d, GROUP)) for d in range(1, GROUP)]

    def signal(sem, devices):
        for to in devices:
            pl.semaphore_signal(sem, inc=1, device_id=to, device_id_type=MESH)

    barrier = pltpu.get_barrier_semaphore()
    signal(barrier, in_y + in_z + in_group)

    def copy(src, dst, sem):
        return pltpu.make_async_copy(src, dst, sem)

    own = [
        copy(dg_h, wbuf.at[zz, yy, pl.ds(0, UNITS)], d_sem.at[0]),
        copy(du_h, wbuf.at[zz, yy, pl.ds(UNITS, UNITS)], d_sem.at[1]),
        copy(dd_h, wbuf.at[zz, yy, pl.ds(2 * UNITS, UNITS)], d_sem.at[2]),
    ]
    proj = [copy(qw_h, qw, w_sem.at[0]), copy(kw_h, kw, w_sem.at[1]), copy(vw_h, vw, w_sem.at[2])]
    outw = [
        copy(
            ow_h.at[pl.ds(h * HEAD, HEAD)],
            ow.at[pl.ds((h % 4) * 2 * HEAD + (h // 4) * HEAD, HEAD)],
            w_sem.at[3 + h],
        )
        for h in range(HEADS)
    ]
    experts = [copy(eg_h.at[0], eg, e_sem.at[0]), copy(eu_h.at[0], eu, e_sem.at[1]), copy(ed_h.at[0], ed, e_sem.at[2])]
    first = [copy(hid_h, hid, s_sem.at[0]), copy(attn_gain_h, attn_gain, s_sem.at[1])]
    scalars = [copy(lens_h, lens, s_sem.at[2]), copy(bias_h, bias, s_sem.at[3])]
    later = [
        copy(ffn_gain_h, ffn_gain, s_sem.at[4]),
        copy(branch_gate_h, branch_gate, s_sem.at[5]),
        copy(routes_h, routes, s_sem.at[6]),
        copy(route_weights_h, route_weights, s_sem.at[7]),
        copy(routes_h, routes_v, s_sem.at[8]),
    ]
    results = [copy(out, out_h, o_sem.at[0]), copy(new_keys, new_keys_h, o_sem.at[1]), copy(new_values, new_values_h, o_sem.at[2])]
    for c in own + first + proj + scalars:
        c.start()

    @pl.loop(0, SEQ)
    def _(b):
        copy(kc_h.at[b], kc.at[b], k_sem.at[b]).start()
        copy(vc_h.at[b], vc.at[b], v_sem.at[b]).start()

    for c in later + outw + experts:
        c.start()

    half = D // 2
    left, right = pl.ds(0, half), pl.ds(half, half)

    def remote(src, dst, s, to):
        return pltpu.make_async_remote_copy(
            src_ref=src, dst_ref=dst, send_sem=snd.at[s], recv_sem=rcv.at[s], device_id=to, device_id_type=MESH
        )

    def push(block, s, to):
        remote(block, block, s, to).start()

    def waited(ref, s):
        copy(ref, ref, snd.at[s]).wait()

    def arrived(ref, s):
        with jax.named_scope(f"arrived_{s}"):
            copy(ref, ref, rcv.at[s]).wait()

    def start_weights():
        with jax.named_scope("barrier_1"):
            pl.semaphore_wait(barrier, len(in_y + in_z + in_group))
        signal(ready.at[0], in_y)
        for c in own:
            c.wait()
        for to in in_y:
            push(wbuf.at[zz, yy, :, left], 0, to)
        for to in in_z:
            push(wbuf.at[zz, yy, :, right], 1, to)
        for to in in_z[:2]:
            push(wbuf.at[zz, yy, :, left], 4, to)
        for to in in_y[:2]:
            push(wbuf.at[zz, yy, :, right], 5, to)

    def blocks_of(a, b):
        return wbuf.at[pl.ds(0, a), pl.ds(0, b), :, left]

    z_by = [lax.rem(zz + d, RING) for d in range(RING)]
    y_by = [lax.rem(yy + d, RING) for d in range(RING)]

    @pl.when(zz == 3)
    def _():
        start_weights()

    row = lax.broadcasted_iota(jnp.int32, (128, 256), 0)
    col = lax.broadcasted_iota(jnp.int32, (128, 256), 1)
    tri[...] = jnp.where((row > col) | (col >= 128), 1.0, 0.0).astype(BF16)

    for c in first:
        c.wait()
    normed = rms_norm(hid[...].astype(F32), attn_gain[...])
    for c in proj:
        c.wait()
    new_keys[...] = dot(normed, kw[...]).astype(BF16)
    new_values[...] = dot(normed, vw[...]).astype(BF16)
    for c in results[1:]:
        c.start()
    queries = dot(normed, qw[...]).astype(BF16).astype(F32)
    low = lax.broadcasted_iota(jnp.int32, (SEQ, 128), 1) < HEAD
    for h in range(HEADS):
        piece = queries[:, (h // 2) * 128 : (h // 2 + 1) * 128]
        if (h % 2) != (h // 4):
            piece = pltpu.roll(piece, HEAD, axis=1)
        piece = jnp.where(low, piece, 0.0) if h < 4 else jnp.where(low, 0.0, piece)
        qs[pl.ds(h, SEQ, stride=HEADS), :] = piece

    @pl.when((zz == 1) | (zz == 2))
    def _():
        start_weights()

    for c in scalars:
        c.wait()
    heads = lax.broadcasted_iota(jnp.int32, (HEADS, LEN), 0)
    bias_v = jnp.zeros((HEADS, LEN), F32)
    for h in range(HEADS):
        bias_v = jnp.where(heads == h, bias[h], bias_v)
    pos = lax.broadcasted_iota(jnp.int32, (HEADS, LEN), 1)
    blocks = LEN // 128

    @jax.named_scope("attend")
    def attend(start, count):
        logs, keeps, lives = [], [], []
        for j in range(count):
            b = start + j
            copy(kc_h.at[b], kc.at[b], k_sem.at[b]).wait()
            q = qs[pl.ds(b * HEADS, HEADS), :].astype(BF16)
            z = nt_dot(q, kc[b]) * (HEAD**-0.5) + bias_v
            live = pos < lens[b]
            t = jnp.log(1.0 + jnp.exp(-jnp.abs(z)))
            logs.append(jnp.minimum(z, 0.0) - t)
            keeps.append(jnp.where(live, jnp.minimum(-z, 0.0) - t, 0.0))
            lives.append(live)
        keep = jnp.concatenate(
            [keeps[j][:, c * 128 : (c + 1) * 128] for j in range(count) for c in range(blocks)], axis=0
        )
        hi = keep.astype(BF16)
        rest = keep - hi.astype(F32)
        mid = rest.astype(BF16)
        lo = (rest - mid.astype(F32)).astype(BF16)
        sums = dot(hi, tri[...]) + dot(mid, tri[...]) + dot(lo, tri[...])
        for j in range(count):
            b = start + j
            beyond = jnp.zeros((HEADS, 128), F32)
            pieces = [None] * blocks
            for c in reversed(range(blocks)):
                at = (j * blocks + c) * HEADS
                after = sums[at : at + HEADS, :128] + beyond
                beyond = beyond + sums[at : at + HEADS, 128:]
                cut = slice(c * 128, (c + 1) * 128)
                pieces[c] = jnp.where(lives[j][:, cut], jnp.exp(logs[j][:, cut] + after), 0.0)
            weights = jnp.concatenate(pieces, axis=1).astype(BF16)
            copy(vc_h.at[b], vc.at[b], v_sem.at[b]).wait()
            os_[pl.ds(b * HEADS, HEADS), :] = dot(weights, vc[b])

    attend(0, 8)

    @pl.when(zz == 0)
    def _():
        start_weights()

    attend(8, 4)
    with jax.named_scope("barrier_2"):
        pl.semaphore_wait(ready.at[0], len(in_y))
    signal(ready.at[1], in_group)

    arrived(blocks_of(1, 3), 0)
    arrived(blocks_of(1, 3), 1)
    for d in (1, 2, 3):
        for to in in_z[:2]:
            push(wbuf.at[zz, y_by[d], :, left], 8, to)
        for to in in_y[:2]:
            push(wbuf.at[z_by[d], yy, :, right], 9, to)

    attend(12, 4)
    with jax.named_scope("barrier_3"):
        pl.semaphore_wait(ready.at[1], len(in_group))

    for c in later + outw:
        c.wait()
    attended = []
    for h in range(4):
        first = os_[pl.ds(h, SEQ, stride=HEADS), :]
        second = os_[pl.ds(h + 4, SEQ, stride=HEADS), :]
        attended.append(jnp.where(low, first, second).astype(BF16))
    middle = hid[...].astype(F32) + dot(jnp.concatenate(attended, axis=1), ow[...])
    mid_s[...] = middle
    ffn_in = rms_norm(middle, ffn_gain[...])
    xg[xx, core] = ffn_in

    experts_i = lax.broadcasted_iota(jnp.int32, (DEV, SEQ), 0)
    hit = routes_v[0:1, :] == experts_i
    for k in range(1, TOP):
        hit = hit | (routes_v[k : k + 1, :] == experts_i)
    pick = jnp.where(hit, 1.0, 0.0).astype(BF16)

    def to_rows(values, c):
        for j in range(values.shape[1] // 128):
            tile32[pl.ds(c + j, DEV, stride=16), :] = values[:, j * 128 : (j + 1) * 128]

    def pack(dst):
        @pl.loop(0, DEV // 8)
        def _(i):
            for j in range(8):
                r = i * 8 + j
                dst[r] = tile32[pl.ds(pl.multiple_of(r * 16, 16), 16), :].astype(BF16)

    def exchange(src, dst, s):
        with jax.named_scope(f"exchange_{s}"):

            @pl.loop(1, DEV)
            def _(d):
                t = lax.rem(me + d, DEV)
                remote(src.at[t], dst.at[me], s, (t,)).start()

    for c in range(0, 16, 4):
        to_rows(dot(pick, ffn_in[:, c * 128 : (c + 4) * 128]), c)
    pack(send1)
    exchange(send1, arr1, 2)
    arr1[me] = send1[me]
    for to in in_x:
        push(xg.at[xx, core], 3, to)

    arrived(blocks_of(1, 2), 4)
    arrived(blocks_of(1, 2), 5)
    push(wbuf.at[z_by[3], yy, :, left], 10, in_z[0])
    push(wbuf.at[zz, y_by[3], :, right], 11, in_y[0])
    arrived(blocks_of(2, 3), 8)
    arrived(blocks_of(2, 3), 9)
    for d, side in ((1, 3), (2, 1), (3, 1)):
        push(wbuf.at[z_by[side], y_by[d], :, left], 12, in_z[0 if side == 3 else 1])
        push(wbuf.at[z_by[d], y_by[side], :, right], 13, in_y[0 if side == 3 else 1])

    for c in experts:
        c.wait()
    most = pl.ds(0, DEV - 1)
    arrived(arr1.at[most], 2)
    arrived(xg.at[pl.ds(0, 3), 0], 3)
    push(xg.at[:, core], 14, sibling)

    @pl.loop(0, DEV // 8)
    def _(i):
        for j in range(8):
            r = i * 8 + j
            tile32[pl.ds(pl.multiple_of(r * 16, 16), 16), :] = arr1[r].astype(F32)

    rows = jnp.concatenate([tile32[pl.ds(c, DEV, stride=16), :].astype(BF16) for c in range(16)], axis=1)
    hidden = (silu(dot(rows, eg[...])) * dot(rows, eu[...])).astype(BF16)
    for c in range(0, 16, 4):
        to_rows(dot(hidden, ed[:, c * 128 : (c + 4) * 128]), c)
    pack(send2)

    exchange(send2, arr2, 6)
    arr2[me] = send2[me]

    arrived(xg.at[:, 0], 14)
    arrived(blocks_of(1, 1), 10)
    arrived(blocks_of(1, 1), 11)
    arrived(blocks_of(1, 3), 12)
    arrived(blocks_of(1, 3), 13)
    tokens = xg[...].reshape(GROUP * SEQ, D)

    def share(n):
        return wbuf[:, :, n * UNITS : (n + 1) * UNITS, :].reshape(RING * RING * UNITS, D)

    dense_hidden = (silu(nt_dot(tokens, share(0))) * nt_dot(tokens, share(1))).astype(BF16)
    part[...] = dot(dense_hidden, share(2)).astype(BF16).reshape(RING, 2, SEQ, D)
    remote(part.at[:, 1 - core], pair_in, 15, sibling).start()
    arrived(pair_in, 15)
    for x in range(RING):
        part2[x] = (part[x, core].astype(F32) + pair_in[x].astype(F32)).astype(BF16)
    for d, to in zip((1, 3, 2), in_x):
        remote(part2.at[lax.rem(xx + d, RING)], parts_in.at[xx], 7, to).start()
    parts_in[xx] = part2[xx]

    ffn_f = xg[xx, core].astype(F32)
    gate_value = jax.nn.sigmoid(jnp.sum(ffn_f * branch_gate[...], axis=-1, keepdims=True))
    arrived(arr2.at[most], 6)
    for t in range(SEQ):
        total = jnp.zeros((16, 128), F32)
        for k in range(TOP):
            total = total + route_weights[k, t] * arr2[routes[k, t]].astype(F32)
        tile32[pl.ds(t * 16, 16), :] = total
    arrived(parts_in.at[pl.ds(0, RING - 1)], 7)
    for c in range(16):
        cut = slice(c * 128, (c + 1) * 128)
        dense = parts_in[0, :, cut].astype(F32)
        for g in range(1, RING):
            dense = dense + parts_in[g, :, cut].astype(F32)
        out[:, cut] = (mid_s[:, cut] + tile32[pl.ds(c, SEQ, stride=16), :] + gate_value * dense).astype(BF16)

    results[0].start()

    with jax.named_scope("sent"):
        for n, many in enumerate(
            (
                blocks_of(1, 3),
                blocks_of(1, 3),
                send1.at[most],
                xg.at[pl.ds(0, 3), 0],
                blocks_of(1, 2),
                blocks_of(1, 2),
                send2.at[most],
                part2.at[pl.ds(0, 3)],
                blocks_of(2, 3),
                blocks_of(2, 3),
                blocks_of(1, 1),
                blocks_of(1, 1),
                blocks_of(1, 3),
                blocks_of(1, 3),
                xg.at[:, 0],
                pair_in,
            )
        ):
            waited(many, n)
        for c in results:
            c.wait()


def hand_on(*arrays):
    n = len(arrays)

    def body(*refs):
        ins, outs, held, sem = refs[:n], refs[n : 2 * n], refs[2 * n : 3 * n], refs[3 * n]
        gets = [pltpu.make_async_copy(ins[i], held[i], sem.at[i]) for i in range(n)]
        puts = [pltpu.make_async_copy(held[i], outs[i], sem.at[n + i]) for i in range(n)]
        for c in gets:
            c.start()
        for g, p in zip(gets, puts):
            g.wait()
            p.start()
        for c in puts:
            c.wait()

    spec = pl.BlockSpec(memory_space=pl.ANY)
    return pl.pallas_call(
        body,
        name="hand_on",
        out_shape=tuple(jax.ShapeDtypeStruct(a.shape, a.dtype) for a in arrays),
        in_specs=[spec] * n,
        out_specs=(spec,) * n,
        scratch_shapes=[pltpu.VMEM(a.shape, a.dtype) for a in arrays] + [pltpu.SemaphoreType.DMA((2 * n,))],
        compiler_params=pltpu.CompilerParams(vmem_limit_bytes=60 * 1024 * 1024),
    )(*arrays)


def per_device(
    hidden_in,
    lengths,
    attn_gain,
    query_weight,
    key_weight,
    value_weight,
    score_bias,
    out_weight,
    key_cache,
    value_cache,
    ffn_gain,
    routes,
    route_weights,
    expert_gate,
    expert_up,
    expert_down,
    dense_gate,
    dense_up,
    dense_down,
    branch_gate,
):
    hbm = pl.BlockSpec(memory_space=pl.ANY)
    dma = pltpu.SemaphoreType.DMA
    return hand_on(
        *pl.pallas_call(
            kernel,
            name="decode_layer",
            out_shape=(
                jax.ShapeDtypeStruct((SEQ, D), BF16),
                jax.ShapeDtypeStruct((SEQ, 128), BF16),
                jax.ShapeDtypeStruct((SEQ, 128), BF16),
            ),
            in_specs=[hbm] * 20,
            out_specs=(hbm, hbm, hbm),
            scratch_shapes=[
                pltpu.SMEM((SEQ,), jnp.int32),
                pltpu.SMEM((HEADS,), F32),
                pltpu.SMEM((TOP, SEQ), jnp.int32),
                pltpu.SMEM((TOP, SEQ), F32),
                pltpu.VMEM((SEQ, D), BF16),
                pltpu.VMEM((1, D), F32),
                pltpu.VMEM((1, D), F32),
                pltpu.VMEM((1, D), F32),
                pltpu.VMEM((TOP, SEQ), jnp.int32),
                pltpu.VMEM((SEQ, D), BF16),
                pltpu.VMEM((SEQ, 128), BF16),
                pltpu.VMEM((SEQ, 128), BF16),
                pltpu.VMEM((D, HEADS * HEAD), BF16),
                pltpu.VMEM((D, 128), BF16),
                pltpu.VMEM((D, 128), BF16),
                pltpu.VMEM((HEADS * HEAD, D), BF16),
                pltpu.VMEM((SEQ, LEN, 128), BF16),
                pltpu.VMEM((SEQ, LEN, 128), BF16),
                pltpu.VMEM((D, EFF), BF16),
                pltpu.VMEM((D, EFF), BF16),
                pltpu.VMEM((EFF, D), BF16),
                pltpu.VMEM((RING, RING, 3 * UNITS, D), BF16),
                pltpu.VMEM((RING, 2, SEQ, D), BF16),
                pltpu.VMEM((RING, 2, SEQ, D), BF16),
                pltpu.VMEM((RING, SEQ, D), BF16),
                pltpu.VMEM((RING, SEQ, D), BF16),
                pltpu.VMEM((RING, SEQ, D), BF16),
                pltpu.VMEM((DEV * 16, 128), F32),
                pltpu.VMEM((DEV, 16, 128), BF16),
                pltpu.VMEM((DEV, 16, 128), BF16),
                pltpu.VMEM((DEV, 16, 128), BF16),
                pltpu.VMEM((DEV, 16, 128), BF16),
                pltpu.VMEM((SEQ * HEADS, 128), F32),
                pltpu.VMEM((SEQ * HEADS, 128), F32),
                pltpu.VMEM((128, 256), BF16),
                pltpu.VMEM((SEQ, D), F32),
                dma((9,)),
                dma((3,)),
                dma((3 + HEADS,)),
                dma((SEQ,)),
                dma((SEQ,)),
                dma((3,)),
                dma((3,)),
                dma((16,)),
                dma((16,)),
                pltpu.SemaphoreType.REGULAR((2,)),
            ],
            compiler_params=pltpu.CompilerParams(
                collective_id=0, has_side_effects=True, vmem_limit_bytes=60 * 1024 * 1024
            ),
        )(
            lengths,
            score_bias,
            routes.T,
            route_weights.T,
            hidden_in,
            attn_gain.reshape(1, D),
            ffn_gain.reshape(1, D),
            branch_gate.reshape(1, D),
            query_weight,
            key_weight,
            value_weight,
            out_weight,
            key_cache,
            value_cache,
            expert_gate,
            expert_up,
            expert_down,
            dense_gate.T,
            dense_up.T,
            dense_down.T,
        )
    )


def solution(mesh):
    return jax.shard_map(
        per_device,
        mesh=mesh,
        in_specs=(
            P("ep", None),
            P("ep"),
            P(),
            P(),
            P(),
            P(),
            P(),
            P(),
            P("ep", None, None),
            P("ep", None, None),
            P(),
            P("ep", None),
            P("ep", None),
            P("ep", None, None),
            P("ep", None, None),
            P("ep", None, None),
            P(None, "ep"),
            P(None, "ep"),
            P(None, "ep"),
            P(),
        ),
        out_specs=(P("ep", None), P("ep", None), P("ep", None)),
        check_vma=False,
    )
```

```python
import itertools

import jax
import jax.numpy as jnp
from jax import lax
from jax.experimental import pallas as pl
from jax.experimental.pallas import tpu as pltpu
from jax.sharding import PartitionSpec as P

AXIS = "ep"
DEV = 128
GROUP = 8
RING = 4
SEQ = 16
D = 2048
LEN = 1024
HEAD = 64
HEADS = 8
TOP = 4
EFF = 512
UNITS = 16
EPS = 1e-06
MESH = pl.DeviceIdType.MESH
BF16 = jnp.bfloat16
FAR_FIRST = sorted(
    (o for o in itertools.product(range(RING), range(RING), range(RING), range(2)) if any(o)),
    key=lambda o: -sum(min(d, RING - d) for d in o[:3]),
)
F32 = jnp.float32


def rms_norm(values, gain):
    scale = lax.rsqrt(jnp.mean(values * values, axis=-1, keepdims=True) + EPS)
    return (values * scale * gain).astype(BF16)


def silu(v):
    return v / (1.0 + jnp.exp(-v))


def nt_dot(a, b):
    return lax.dot_general(a, b, (((1,), (1,)), ((), ())), preferred_element_type=F32)


def dot(a, b):
    return jnp.dot(a, b, preferred_element_type=F32)


def kernel(
    lens_h,
    bias_h,
    routes_h,
    route_weights_h,
    hid_h,
    attn_gain_h,
    ffn_gain_h,
    branch_gate_h,
    qw_h,
    kw_h,
    vw_h,
    ow_h,
    kc_h,
    vc_h,
    eg_h,
    eu_h,
    ed_h,
    dg_h,
    du_h,
    dd_h,
    out_h,
    new_keys_h,
    new_values_h,
    lens,
    bias,
    routes,
    route_weights,
    hid,
    attn_gain,
    ffn_gain,
    branch_gate,
    routes_v,
    out,
    new_keys,
    new_values,
    qw,
    kw,
    vw,
    ow,
    kc,
    vc,
    eg,
    eu,
    ed,
    wbuf,
    xg,
    part,
    part2,
    pair_in,
    parts_in,
    tile32,
    send1,
    arr1,
    send2,
    arr2,
    qs,
    os_,
    tri,
    mid_s,
    s_sem,
    o_sem,
    w_sem,
    k_sem,
    v_sem,
    e_sem,
    d_sem,
    snd,
    rcv,
    ready,
):
    me = lax.axis_index(AXIS)
    grp = me // GROUP
    mem = lax.rem(me, GROUP)
    zz = grp // RING
    yy = lax.rem(grp, RING)

    def device(z, y, member):
        return ((z * RING + y) * GROUP + member,)

    in_y = [device(zz, lax.rem(yy + d, RING), mem) for d in (1, 3, 2)]
    in_z = [device(lax.rem(zz + d, RING), yy, mem) for d in (1, 3, 2)]
    xx, core = mem // 2, lax.rem(mem, 2)
    in_x = [device(zz, yy, lax.rem(xx + d, RING) * 2 + core) for d in (1, 3, 2)]
    sibling = device(zz, yy, xx * 2 + 1 - core)
    in_group = [device(zz, yy, lax.rem(mem + d, GROUP)) for d in range(1, GROUP)]

    def signal(sem, devices):
        for to in devices:
            pl.semaphore_signal(sem, inc=1, device_id=to, device_id_type=MESH)

    barrier = pltpu.get_barrier_semaphore()
    signal(barrier, in_y + in_z + in_group)

    def copy(src, dst, sem):
        return pltpu.make_async_copy(src, dst, sem)

    own = [
        copy(dg_h, wbuf.at[zz, yy, pl.ds(0, UNITS)], d_sem.at[0]),
        copy(du_h, wbuf.at[zz, yy, pl.ds(UNITS, UNITS)], d_sem.at[1]),
        copy(dd_h, wbuf.at[zz, yy, pl.ds(2 * UNITS, UNITS)], d_sem.at[2]),
    ]
    proj = [copy(qw_h, qw, w_sem.at[0]), copy(kw_h, kw, w_sem.at[1]), copy(vw_h, vw, w_sem.at[2])]
    outw = [
        copy(
            ow_h.at[pl.ds(h * HEAD, HEAD)],
            ow.at[pl.ds((h % 4) * 2 * HEAD + (h // 4) * HEAD, HEAD)],
            w_sem.at[3 + h],
        )
        for h in range(HEADS)
    ]
    experts = [copy(eg_h.at[0], eg, e_sem.at[0]), copy(eu_h.at[0], eu, e_sem.at[1]), copy(ed_h.at[0], ed, e_sem.at[2])]
    first = [copy(hid_h, hid, s_sem.at[0]), copy(attn_gain_h, attn_gain, s_sem.at[1])]
    scalars = [copy(lens_h, lens, s_sem.at[2]), copy(bias_h, bias, s_sem.at[3])]
    later = [
        copy(ffn_gain_h, ffn_gain, s_sem.at[4]),
        copy(branch_gate_h, branch_gate, s_sem.at[5]),
        copy(routes_h, routes, s_sem.at[6]),
        copy(route_weights_h, route_weights, s_sem.at[7]),
        copy(routes_h, routes_v, s_sem.at[8]),
    ]
    results = [copy(out, out_h, o_sem.at[0]), copy(new_keys, new_keys_h, o_sem.at[1]), copy(new_values, new_values_h, o_sem.at[2])]
    for c in own + first + proj + scalars:
        c.start()

    for first_b in (0, 8):

        @pl.loop(first_b, first_b + 8)
        def _(b):
            copy(kc_h.at[b], kc.at[b], k_sem.at[b]).start()

        @pl.loop(first_b, first_b + 8)
        def _(b):
            copy(vc_h.at[b], vc.at[b], v_sem.at[b]).start()

    for c in later + outw + experts:
        c.start()

    half = D // 2
    left, right = pl.ds(0, half), pl.ds(half, half)

    def remote(src, dst, s, to):
        return pltpu.make_async_remote_copy(
            src_ref=src, dst_ref=dst, send_sem=snd.at[s], recv_sem=rcv.at[s], device_id=to, device_id_type=MESH
        )

    def push(block, s, to):
        remote(block, block, s, to).start()

    def waited(ref, s):
        copy(ref, ref, snd.at[s]).wait()

    def arrived(ref, s):
        with jax.named_scope(f"arrived_{s}"):
            copy(ref, ref, rcv.at[s]).wait()

    def start_weights():
        with jax.named_scope("barrier_1"):
            pl.semaphore_wait(barrier, len(in_y + in_z + in_group))
        signal(ready.at[0], in_y)
        for c in own:
            c.wait()
        for to in in_y:
            push(wbuf.at[zz, yy, :, left], 0, to)
        for to in in_z:
            push(wbuf.at[zz, yy, :, right], 1, to)
        for to in in_z[:2]:
            push(wbuf.at[zz, yy, :, left], 4, to)
        for to in in_y[:2]:
            push(wbuf.at[zz, yy, :, right], 5, to)

    def blocks_of(a, b):
        return wbuf.at[pl.ds(0, a), pl.ds(0, b), :, left]

    x_by = [lax.rem(xx + d, RING) for d in range(RING)]
    core_by = [core, 1 - core]
    z_by = [lax.rem(zz + d, RING) for d in range(RING)]
    y_by = [lax.rem(yy + d, RING) for d in range(RING)]

    @pl.when(zz == 3)
    def _():
        start_weights()

    row = lax.broadcasted_iota(jnp.int32, (128, 256), 0)
    col = lax.broadcasted_iota(jnp.int32, (128, 256), 1)
    tri[...] = jnp.where((row > col) | (col >= 128), 1.0, 0.0).astype(BF16)

    for c in first:
        c.wait()
    normed = rms_norm(hid[...].astype(F32), attn_gain[...])
    for c in proj:
        c.wait()
    new_keys[...] = dot(normed, kw[...]).astype(BF16)
    new_values[...] = dot(normed, vw[...]).astype(BF16)
    for c in results[1:]:
        c.start()
    queries = dot(normed, qw[...]).astype(BF16).astype(F32)
    low = lax.broadcasted_iota(jnp.int32, (SEQ, 128), 1) < HEAD
    for h in range(HEADS):
        piece = queries[:, (h // 2) * 128 : (h // 2 + 1) * 128]
        if (h % 2) != (h // 4):
            piece = pltpu.roll(piece, HEAD, axis=1)
        piece = jnp.where(low, piece, 0.0) if h < 4 else jnp.where(low, 0.0, piece)
        qs[pl.ds(h, SEQ, stride=HEADS), :] = piece

    @pl.when((zz == 1) | (zz == 2))
    def _():
        start_weights()

    for c in scalars:
        c.wait()
    heads = lax.broadcasted_iota(jnp.int32, (HEADS, LEN), 0)
    bias_v = jnp.zeros((HEADS, LEN), F32)
    for h in range(HEADS):
        bias_v = jnp.where(heads == h, bias[h], bias_v)
    pos = lax.broadcasted_iota(jnp.int32, (HEADS, LEN), 1)
    blocks = LEN // 128

    @jax.named_scope("attend")
    def attend(start, count):
        logs, keeps, lives = [], [], []
        for b in range(start, start + count):
            copy(kc_h.at[b], kc.at[b], k_sem.at[b]).wait()
        for b in range(start, start + count):
            copy(vc_h.at[b], vc.at[b], v_sem.at[b]).wait()
        for j in range(count):
            b = start + j
            q = qs[pl.ds(b * HEADS, HEADS), :].astype(BF16)
            z = nt_dot(q, kc[b]) * (HEAD**-0.5) + bias_v
            live = pos < lens[b]
            t = jnp.log(1.0 + jnp.exp(-jnp.abs(z)))
            logs.append(jnp.minimum(z, 0.0) - t)
            keeps.append(jnp.where(live, jnp.minimum(-z, 0.0) - t, 0.0))
            lives.append(live)
        keep = jnp.concatenate(
            [keeps[j][:, c * 128 : (c + 1) * 128] for j in range(count) for c in range(blocks)], axis=0
        )
        hi = keep.astype(BF16)
        rest = keep - hi.astype(F32)
        mid = rest.astype(BF16)
        lo = (rest - mid.astype(F32)).astype(BF16)
        sums = dot(hi, tri[...]) + dot(mid, tri[...]) + dot(lo, tri[...])
        for j in range(count):
            b = start + j
            beyond = jnp.zeros((HEADS, 128), F32)
            pieces = [None] * blocks
            for c in reversed(range(blocks)):
                at = (j * blocks + c) * HEADS
                after = sums[at : at + HEADS, :128] + beyond
                beyond = beyond + sums[at : at + HEADS, 128:]
                cut = slice(c * 128, (c + 1) * 128)
                pieces[c] = jnp.where(lives[j][:, cut], jnp.exp(logs[j][:, cut] + after), 0.0)
            weights = jnp.concatenate(pieces, axis=1).astype(BF16)
            os_[pl.ds(b * HEADS, HEADS), :] = dot(weights, vc[b])

    attend(0, 8)

    @pl.when(zz == 0)
    def _():
        start_weights()

    attend(8, 8)
    with jax.named_scope("barrier_2"):
        pl.semaphore_wait(ready.at[0], len(in_y))
    signal(ready.at[1], in_group)

    for c in later + outw:
        c.wait()
    attended = []
    for h in range(4):
        first = os_[pl.ds(h, SEQ, stride=HEADS), :]
        second = os_[pl.ds(h + 4, SEQ, stride=HEADS), :]
        attended.append(jnp.where(low, first, second).astype(BF16))
    middle = hid[...].astype(F32) + dot(jnp.concatenate(attended, axis=1), ow[...])
    mid_s[...] = middle
    ffn_in = rms_norm(middle, ffn_gain[...])
    xg[xx, core] = ffn_in

    experts_i = lax.broadcasted_iota(jnp.int32, (DEV, SEQ), 0)
    hit = routes_v[0:1, :] == experts_i
    for k in range(1, TOP):
        hit = hit | (routes_v[k : k + 1, :] == experts_i)
    pick = jnp.where(hit, 1.0, 0.0).astype(BF16)

    def to_rows(values, c):
        for j in range(values.shape[1] // 128):
            tile32[pl.ds(c + j, DEV, stride=16), :] = values[:, j * 128 : (j + 1) * 128]

    def pack(dst):
        @pl.loop(0, DEV // 8)
        def _(i):
            for j in range(8):
                r = i * 8 + j
                dst[r] = tile32[pl.ds(pl.multiple_of(r * 16, 16), 16), :].astype(BF16)

    def exchange(src, dst, s):
        with jax.named_scope(f"exchange_{s}"):

            for dz, dy, dx, dc in FAR_FIRST:
                t = ((z_by[dz] * RING + y_by[dy]) * RING + x_by[dx]) * 2 + core_by[dc]
                remote(src.at[t], dst.at[me], s, (t,)).start()

    for c in range(0, 16, 4):
        to_rows(dot(pick, ffn_in[:, c * 128 : (c + 4) * 128]), c)
    pack(send1)
    with jax.named_scope("barrier_3"):
        pl.semaphore_wait(ready.at[1], len(in_group))

    exchange(send1, arr1, 2)
    arr1[me] = send1[me]
    for to in in_x:
        push(xg.at[xx, core], 3, to)

    second = {1: (8, 9), 2: (16, 17), 3: (18, 19)}
    third = {0: (10, 11), 1: (12, 13), 2: (20, 21), 3: (22, 23)}

    arrived(blocks_of(1, 3), 0)
    arrived(blocks_of(1, 3), 1)
    for d in (1, 2, 3):
        for to in in_z[:2]:
            push(wbuf.at[zz, y_by[d], :, left], second[d][0], to)
        for to in in_y[:2]:
            push(wbuf.at[z_by[d], yy, :, right], second[d][1], to)

    arrived(blocks_of(1, 2), 4)
    arrived(blocks_of(1, 2), 5)
    push(wbuf.at[z_by[3], yy, :, left], 10, in_z[0])
    push(wbuf.at[zz, y_by[3], :, right], 11, in_y[0])
    def relay(d):
        arrived(blocks_of(1, 2), second[d][0])
        arrived(blocks_of(1, 2), second[d][1])
        side = 3 if d == 1 else 1
        push(wbuf.at[z_by[side], y_by[d], :, left], third[d][0], in_z[0 if side == 3 else 1])
        push(wbuf.at[z_by[d], y_by[side], :, right], third[d][1], in_y[0 if side == 3 else 1])

    for c in experts:
        c.wait()
    most = pl.ds(0, DEV - 1)
    arrived(arr1.at[most], 2)
    arrived(xg.at[pl.ds(0, 3), 0], 3)
    push(xg.at[:, core], 14, sibling)

    @pl.loop(0, DEV // 8)
    def _(i):
        for j in range(8):
            r = i * 8 + j
            tile32[pl.ds(pl.multiple_of(r * 16, 16), 16), :] = arr1[r].astype(F32)

    rows = jnp.concatenate([tile32[pl.ds(c, DEV, stride=16), :].astype(BF16) for c in range(16)], axis=1)
    hidden = (silu(dot(rows, eg[...])) * dot(rows, eu[...])).astype(BF16)
    for c in range(0, 16, 4):
        to_rows(dot(hidden, ed[:, c * 128 : (c + 4) * 128]), c)
    pack(send2)

    for d in (1, 2, 3):
        relay(d)
    for n in third[0]:
        arrived(blocks_of(1, 1), n)
    for n in third[1]:
        arrived(blocks_of(1, 1), n)
    for n in third[2]:
        arrived(blocks_of(1, 1), n)
    exchange(send2, arr2, 6)
    arr2[me] = send2[me]

    arrived(xg.at[:, 0], 14)
    for n in third[3]:
        arrived(blocks_of(1, 1), n)
    tokens = xg[...].reshape(GROUP * SEQ, D)

    def share(n):
        return wbuf[:, :, n * UNITS : (n + 1) * UNITS, :].reshape(RING * RING * UNITS, D)

    dense_hidden = (silu(nt_dot(tokens, share(0))) * nt_dot(tokens, share(1))).astype(BF16)
    for n, cols in enumerate((left, right)):
        part[:, :, :, cols] = dot(dense_hidden, share(2)[:, n * half : (n + 1) * half]).astype(BF16).reshape(RING, 2, SEQ, half)
        remote(part.at[:, 1 - core, :, cols], pair_in.at[:, :, cols], (15, 24)[n], sibling).start()
    for n, cols in enumerate((left, right)):
        arrived(pair_in.at[:, :, cols], (15, 24)[n])
        for x in range(RING):
            part2[x, :, cols] = (part[x, core, :, cols].astype(F32) + pair_in[x, :, cols].astype(F32)).astype(BF16)
        for d, to in zip((1, 3, 2), in_x):
            remote(part2.at[x_by[d], :, cols], parts_in.at[xx, :, cols], (7, 25)[n], to).start()
    parts_in[xx] = part2[xx]

    ffn_f = xg[xx, core].astype(F32)
    gate_value = jax.nn.sigmoid(jnp.sum(ffn_f * branch_gate[...], axis=-1, keepdims=True))
    arrived(arr2.at[most], 6)
    for t in range(SEQ):
        total = jnp.zeros((16, 128), F32)
        for k in range(TOP):
            total = total + route_weights[k, t] * arr2[routes[k, t]].astype(F32)
        tile32[pl.ds(t * 16, 16), :] = total
    for c in range(16):
        if c % 8 == 0:
            arrived(parts_in.at[pl.ds(0, RING - 1), :, (left, right)[c // 8]], (7, 25)[c // 8])
        cut = slice(c * 128, (c + 1) * 128)
        dense = parts_in[0, :, cut].astype(F32)
        for g in range(1, RING):
            dense = dense + parts_in[g, :, cut].astype(F32)
        out[:, cut] = (mid_s[:, cut] + tile32[pl.ds(c, SEQ, stride=16), :] + gate_value * dense).astype(BF16)

    results[0].start()

    with jax.named_scope("sent"):
        for n, many in enumerate(
            (
                blocks_of(1, 3),
                blocks_of(1, 3),
                send1.at[most],
                xg.at[pl.ds(0, 3), 0],
                blocks_of(1, 2),
                blocks_of(1, 2),
                send2.at[most],
                part2.at[pl.ds(0, 3), :, left],
                blocks_of(1, 2),
                blocks_of(1, 2),
                blocks_of(1, 1),
                blocks_of(1, 1),
                blocks_of(1, 1),
                blocks_of(1, 1),
                xg.at[:, 0],
                pair_in.at[:, :, left],
                blocks_of(1, 2),
                blocks_of(1, 2),
                blocks_of(1, 2),
                blocks_of(1, 2),
                blocks_of(1, 1),
                blocks_of(1, 1),
                blocks_of(1, 1),
                blocks_of(1, 1),
                pair_in.at[:, :, left],
                part2.at[pl.ds(0, 3), :, left],
            )
        ):
            waited(many, n)
        for c in results:
            c.wait()


def hand_on(*arrays):
    n = len(arrays)

    def body(*refs):
        ins, outs, held, sem = refs[:n], refs[n : 2 * n], refs[2 * n : 3 * n], refs[3 * n]
        gets = [pltpu.make_async_copy(ins[i], held[i], sem.at[i]) for i in range(n)]
        puts = [pltpu.make_async_copy(held[i], outs[i], sem.at[n + i]) for i in range(n)]
        for c in gets:
            c.start()
        for g, p in zip(gets, puts):
            g.wait()
            p.start()
        for c in puts:
            c.wait()

    spec = pl.BlockSpec(memory_space=pl.ANY)
    return pl.pallas_call(
        body,
        name="hand_on",
        out_shape=tuple(jax.ShapeDtypeStruct(a.shape, a.dtype) for a in arrays),
        in_specs=[spec] * n,
        out_specs=(spec,) * n,
        scratch_shapes=[pltpu.VMEM(a.shape, a.dtype) for a in arrays] + [pltpu.SemaphoreType.DMA((2 * n,))],
        compiler_params=pltpu.CompilerParams(vmem_limit_bytes=60 * 1024 * 1024),
    )(*arrays)


def per_device(
    hidden_in,
    lengths,
    attn_gain,
    query_weight,
    key_weight,
    value_weight,
    score_bias,
    out_weight,
    key_cache,
    value_cache,
    ffn_gain,
    routes,
    route_weights,
    expert_gate,
    expert_up,
    expert_down,
    dense_gate,
    dense_up,
    dense_down,
    branch_gate,
):
    hbm = pl.BlockSpec(memory_space=pl.ANY)
    dma = pltpu.SemaphoreType.DMA
    return hand_on(
        *pl.pallas_call(
            kernel,
            name="decode_layer",
            out_shape=(
                jax.ShapeDtypeStruct((SEQ, D), BF16),
                jax.ShapeDtypeStruct((SEQ, 128), BF16),
                jax.ShapeDtypeStruct((SEQ, 128), BF16),
            ),
            in_specs=[hbm] * 20,
            out_specs=(hbm, hbm, hbm),
            scratch_shapes=[
                pltpu.SMEM((SEQ,), jnp.int32),
                pltpu.SMEM((HEADS,), F32),
                pltpu.SMEM((TOP, SEQ), jnp.int32),
                pltpu.SMEM((TOP, SEQ), F32),
                pltpu.VMEM((SEQ, D), BF16),
                pltpu.VMEM((1, D), F32),
                pltpu.VMEM((1, D), F32),
                pltpu.VMEM((1, D), F32),
                pltpu.VMEM((TOP, SEQ), jnp.int32),
                pltpu.VMEM((SEQ, D), BF16),
                pltpu.VMEM((SEQ, 128), BF16),
                pltpu.VMEM((SEQ, 128), BF16),
                pltpu.VMEM((D, HEADS * HEAD), BF16),
                pltpu.VMEM((D, 128), BF16),
                pltpu.VMEM((D, 128), BF16),
                pltpu.VMEM((HEADS * HEAD, D), BF16),
                pltpu.VMEM((SEQ, LEN, 128), BF16),
                pltpu.VMEM((SEQ, LEN, 128), BF16),
                pltpu.VMEM((D, EFF), BF16),
                pltpu.VMEM((D, EFF), BF16),
                pltpu.VMEM((EFF, D), BF16),
                pltpu.VMEM((RING, RING, 3 * UNITS, D), BF16),
                pltpu.VMEM((RING, 2, SEQ, D), BF16),
                pltpu.VMEM((RING, 2, SEQ, D), BF16),
                pltpu.VMEM((RING, SEQ, D), BF16),
                pltpu.VMEM((RING, SEQ, D), BF16),
                pltpu.VMEM((RING, SEQ, D), BF16),
                pltpu.VMEM((DEV * 16, 128), F32),
                pltpu.VMEM((DEV, 16, 128), BF16),
                pltpu.VMEM((DEV, 16, 128), BF16),
                pltpu.VMEM((DEV, 16, 128), BF16),
                pltpu.VMEM((DEV, 16, 128), BF16),
                pltpu.VMEM((SEQ * HEADS, 128), F32),
                pltpu.VMEM((SEQ * HEADS, 128), F32),
                pltpu.VMEM((128, 256), BF16),
                pltpu.VMEM((SEQ, D), F32),
                dma((9,)),
                dma((3,)),
                dma((3 + HEADS,)),
                dma((SEQ,)),
                dma((SEQ,)),
                dma((3,)),
                dma((3,)),
                dma((26,)),
                dma((26,)),
                pltpu.SemaphoreType.REGULAR((2,)),
            ],
            compiler_params=pltpu.CompilerParams(
                collective_id=0, has_side_effects=True, vmem_limit_bytes=60 * 1024 * 1024
            ),
        )(
            lengths,
            score_bias,
            routes.T,
            route_weights.T,
            hidden_in,
            attn_gain.reshape(1, D),
            ffn_gain.reshape(1, D),
            branch_gate.reshape(1, D),
            query_weight,
            key_weight,
            value_weight,
            out_weight,
            key_cache,
            value_cache,
            expert_gate,
            expert_up,
            expert_down,
            dense_gate.T,
            dense_up.T,
            dense_down.T,
        )
    )


def solution(mesh):
    return jax.shard_map(
        per_device,
        mesh=mesh,
        in_specs=(
            P("ep", None),
            P("ep"),
            P(),
            P(),
            P(),
            P(),
            P(),
            P(),
            P("ep", None, None),
            P("ep", None, None),
            P(),
            P("ep", None),
            P("ep", None),
            P("ep", None, None),
            P("ep", None, None),
            P("ep", None, None),
            P(None, "ep"),
            P(None, "ep"),
            P(None, "ep"),
            P(),
        ),
        out_specs=(P("ep", None), P("ep", None), P("ep", None)),
        check_vma=False,
    )
```

```python
import itertools

import jax
import jax.numpy as jnp
from jax import lax
from jax.experimental import pallas as pl
from jax.experimental.pallas import tpu as pltpu
from jax.sharding import PartitionSpec as P

AXIS = "ep"
DEV = 128
GROUP = 8
RING = 4
SEQ = 16
D = 2048
LEN = 1024
HEAD = 64
HEADS = 8
TOP = 4
EFF = 512
UNITS = 16
EPS = 1e-06
MESH = pl.DeviceIdType.MESH
BF16 = jnp.bfloat16
FAR_FIRST = sorted(
    (o for o in itertools.product(range(RING), range(RING), range(RING), range(2)) if any(o)),
    key=lambda o: -sum(min(d, RING - d) for d in o[:3]),
)
F32 = jnp.float32


def rms_norm(values, gain):
    scale = lax.rsqrt(jnp.mean(values * values, axis=-1, keepdims=True) + EPS)
    return (values * scale * gain).astype(BF16)


def silu(v):
    return v / (1.0 + jnp.exp(-v))


def nt_dot(a, b):
    return lax.dot_general(a, b, (((1,), (1,)), ((), ())), preferred_element_type=F32)


def dot(a, b):
    return jnp.dot(a, b, preferred_element_type=F32)


def kernel(
    lens_h,
    bias_h,
    routes_h,
    route_weights_h,
    hid_h,
    attn_gain_h,
    ffn_gain_h,
    branch_gate_h,
    qw_h,
    kw_h,
    vw_h,
    ow_h,
    kc_h,
    vc_h,
    eg_h,
    eu_h,
    ed_h,
    dg_h,
    du_h,
    dd_h,
    out_h,
    new_keys_h,
    new_values_h,
    lens,
    bias,
    routes,
    route_weights,
    hid,
    attn_gain,
    ffn_gain,
    branch_gate,
    routes_v,
    out,
    new_keys,
    new_values,
    qw,
    kw,
    vw,
    ow,
    kc,
    vc,
    eg,
    eu,
    ed,
    wbuf,
    xg,
    part,
    part2,
    pair_in,
    parts_in,
    tile32,
    send1,
    arr1,
    send2,
    arr2,
    qs,
    os_,
    tri,
    mid_s,
    s_sem,
    o_sem,
    w_sem,
    k_sem,
    v_sem,
    e_sem,
    d_sem,
    snd,
    rcv,
    ready,
):
    me = lax.axis_index(AXIS)
    grp = me // GROUP
    mem = lax.rem(me, GROUP)
    zz = grp // RING
    yy = lax.rem(grp, RING)

    def device(z, y, member):
        return ((z * RING + y) * GROUP + member,)

    in_y = [device(zz, lax.rem(yy + d, RING), mem) for d in (1, 3, 2)]
    in_z = [device(lax.rem(zz + d, RING), yy, mem) for d in (1, 3, 2)]
    xx, core = mem // 2, lax.rem(mem, 2)
    in_x = [device(zz, yy, lax.rem(xx + d, RING) * 2 + core) for d in (1, 3, 2)]
    sibling = device(zz, yy, xx * 2 + 1 - core)
    in_group = [device(zz, yy, lax.rem(mem + d, GROUP)) for d in range(1, GROUP)]

    def signal(sem, devices):
        for to in devices:
            pl.semaphore_signal(sem, inc=1, device_id=to, device_id_type=MESH)

    barrier = pltpu.get_barrier_semaphore()
    signal(barrier, in_y + in_z + in_group)

    def copy(src, dst, sem):
        return pltpu.make_async_copy(src, dst, sem)

    own = [
        copy(dg_h, wbuf.at[zz, yy, pl.ds(0, UNITS)], d_sem.at[0]),
        copy(du_h, wbuf.at[zz, yy, pl.ds(UNITS, UNITS)], d_sem.at[1]),
        copy(dd_h, wbuf.at[zz, yy, pl.ds(2 * UNITS, UNITS)], d_sem.at[2]),
    ]
    proj = [copy(qw_h, qw, w_sem.at[0]), copy(kw_h, kw, w_sem.at[1]), copy(vw_h, vw, w_sem.at[2])]
    outw = [
        copy(
            ow_h.at[pl.ds(h * HEAD, HEAD)],
            ow.at[pl.ds((h % 4) * 2 * HEAD + (h // 4) * HEAD, HEAD)],
            w_sem.at[3 + h],
        )
        for h in range(HEADS)
    ]
    experts = [copy(eg_h.at[0], eg, e_sem.at[0]), copy(eu_h.at[0], eu, e_sem.at[1]), copy(ed_h.at[0], ed, e_sem.at[2])]
    first = [copy(hid_h, hid, s_sem.at[0]), copy(attn_gain_h, attn_gain, s_sem.at[1])]
    scalars = [copy(lens_h, lens, s_sem.at[2]), copy(bias_h, bias, s_sem.at[3])]
    later = [
        copy(ffn_gain_h, ffn_gain, s_sem.at[4]),
        copy(branch_gate_h, branch_gate, s_sem.at[5]),
        copy(routes_h, routes, s_sem.at[6]),
        copy(route_weights_h, route_weights, s_sem.at[7]),
        copy(routes_h, routes_v, s_sem.at[8]),
    ]
    results = [copy(out, out_h, o_sem.at[0]), copy(new_keys, new_keys_h, o_sem.at[1]), copy(new_values, new_values_h, o_sem.at[2])]
    for c in own + first + proj + scalars:
        c.start()

    for first_b in (0, 8):

        @pl.loop(first_b, first_b + 8)
        def _(b):
            copy(kc_h.at[b], kc.at[b], k_sem.at[b]).start()

        @pl.loop(first_b, first_b + 8)
        def _(b):
            copy(vc_h.at[b], vc.at[b], v_sem.at[b]).start()

    for c in later + outw + experts:
        c.start()

    half = D // 2
    left, right = pl.ds(0, half), pl.ds(half, half)

    def remote(src, dst, s, to):
        return pltpu.make_async_remote_copy(
            src_ref=src, dst_ref=dst, send_sem=snd.at[s], recv_sem=rcv.at[s], device_id=to, device_id_type=MESH
        )

    def push(block, s, to):
        remote(block, block, s, to).start()

    def waited(ref, s):
        copy(ref, ref, snd.at[s]).wait()

    def arrived(ref, s):
        with jax.named_scope(f"arrived_{s}"):
            copy(ref, ref, rcv.at[s]).wait()

    def start_weights():
        with jax.named_scope("barrier_1"):
            pl.semaphore_wait(barrier, len(in_y + in_z + in_group))
        signal(ready.at[0], in_y)
        for c in own:
            c.wait()
        for to in in_y[:2]:
            push(wbuf.at[zz, yy, :, left], 0, to)
        for to in in_z[:2]:
            push(wbuf.at[zz, yy, :, right], 1, to)
        for to in in_z[:2]:
            push(wbuf.at[zz, yy, :, left], 4, to)
        for to in in_y[:2]:
            push(wbuf.at[zz, yy, :, right], 5, to)

    def blocks_of(a, b):
        return wbuf.at[pl.ds(0, a), pl.ds(0, b), :, left]

    x_by = [lax.rem(xx + d, RING) for d in range(RING)]
    core_by = [core, 1 - core]
    z_by = [lax.rem(zz + d, RING) for d in range(RING)]
    y_by = [lax.rem(yy + d, RING) for d in range(RING)]

    @pl.when(zz == 3)
    def _():
        start_weights()

    row = lax.broadcasted_iota(jnp.int32, (128, 256), 0)
    col = lax.broadcasted_iota(jnp.int32, (128, 256), 1)
    tri[...] = jnp.where((row > col) | (col >= 128), 1.0, 0.0).astype(BF16)

    for c in first:
        c.wait()
    normed = rms_norm(hid[...].astype(F32), attn_gain[...])
    for c in proj:
        c.wait()
    new_keys[...] = dot(normed, kw[...]).astype(BF16)
    new_values[...] = dot(normed, vw[...]).astype(BF16)
    for c in results[1:]:
        c.start()
    queries = dot(normed, qw[...]).astype(BF16).astype(F32)
    low = lax.broadcasted_iota(jnp.int32, (SEQ, 128), 1) < HEAD
    for h in range(HEADS):
        piece = queries[:, (h // 2) * 128 : (h // 2 + 1) * 128]
        if (h % 2) != (h // 4):
            piece = pltpu.roll(piece, HEAD, axis=1)
        piece = jnp.where(low, piece, 0.0) if h < 4 else jnp.where(low, 0.0, piece)
        qs[pl.ds(h, SEQ, stride=HEADS), :] = piece

    @pl.when((zz == 1) | (zz == 2))
    def _():
        start_weights()

    for c in scalars:
        c.wait()
    heads = lax.broadcasted_iota(jnp.int32, (HEADS, LEN), 0)
    bias_v = jnp.zeros((HEADS, LEN), F32)
    for h in range(HEADS):
        bias_v = jnp.where(heads == h, bias[h], bias_v)
    pos = lax.broadcasted_iota(jnp.int32, (HEADS, LEN), 1)
    blocks = LEN // 128

    @jax.named_scope("attend")
    def attend(start, count):
        logs, keeps, lives = [], [], []
        for b in range(start, start + count):
            copy(kc_h.at[b], kc.at[b], k_sem.at[b]).wait()
        for b in range(start, start + count):
            copy(vc_h.at[b], vc.at[b], v_sem.at[b]).wait()
        for j in range(count):
            b = start + j
            q = qs[pl.ds(b * HEADS, HEADS), :].astype(BF16)
            z = nt_dot(q, kc[b]) * (HEAD**-0.5) + bias_v
            live = pos < lens[b]
            t = jnp.log(1.0 + jnp.exp(-jnp.abs(z)))
            logs.append(jnp.minimum(z, 0.0) - t)
            keeps.append(jnp.where(live, jnp.minimum(-z, 0.0) - t, 0.0))
            lives.append(live)
        keep = jnp.concatenate(
            [keeps[j][:, c * 128 : (c + 1) * 128] for j in range(count) for c in range(blocks)], axis=0
        )
        hi = keep.astype(BF16)
        rest = keep - hi.astype(F32)
        mid = rest.astype(BF16)
        lo = (rest - mid.astype(F32)).astype(BF16)
        sums = dot(hi, tri[...]) + dot(mid, tri[...]) + dot(lo, tri[...])
        for j in range(count):
            b = start + j
            beyond = jnp.zeros((HEADS, 128), F32)
            pieces = [None] * blocks
            for c in reversed(range(blocks)):
                at = (j * blocks + c) * HEADS
                after = sums[at : at + HEADS, :128] + beyond
                beyond = beyond + sums[at : at + HEADS, 128:]
                cut = slice(c * 128, (c + 1) * 128)
                pieces[c] = jnp.where(lives[j][:, cut], jnp.exp(logs[j][:, cut] + after), 0.0)
            weights = jnp.concatenate(pieces, axis=1).astype(BF16)
            os_[pl.ds(b * HEADS, HEADS), :] = dot(weights, vc[b])

    attend(0, 8)

    @pl.when(zz == 0)
    def _():
        start_weights()

    attend(8, 8)
    with jax.named_scope("barrier_2"):
        pl.semaphore_wait(ready.at[0], len(in_y))
    signal(ready.at[1], in_group)

    for c in later + outw:
        c.wait()
    attended = []
    for h in range(4):
        first = os_[pl.ds(h, SEQ, stride=HEADS), :]
        second = os_[pl.ds(h + 4, SEQ, stride=HEADS), :]
        attended.append(jnp.where(low, first, second).astype(BF16))
    middle = hid[...].astype(F32) + dot(jnp.concatenate(attended, axis=1), ow[...])
    mid_s[...] = middle
    ffn_in = rms_norm(middle, ffn_gain[...])
    xg[xx, core] = ffn_in

    experts_i = lax.broadcasted_iota(jnp.int32, (DEV, SEQ), 0)
    hit = routes_v[0:1, :] == experts_i
    for k in range(1, TOP):
        hit = hit | (routes_v[k : k + 1, :] == experts_i)
    pick = jnp.where(hit, 1.0, 0.0).astype(BF16)

    def to_rows(values, c):
        for j in range(values.shape[1] // 128):
            tile32[pl.ds(c + j, DEV, stride=16), :] = values[:, j * 128 : (j + 1) * 128]

    def pack(dst):
        @pl.loop(0, DEV // 8)
        def _(i):
            for j in range(8):
                r = i * 8 + j
                dst[r] = tile32[pl.ds(pl.multiple_of(r * 16, 16), 16), :].astype(BF16)

    def exchange(src, dst, s, order=FAR_FIRST):
        with jax.named_scope(f"exchange_{s}"):

            for dz, dy, dx, dc in order:
                t = ((z_by[dz] * RING + y_by[dy]) * RING + x_by[dx]) * 2 + core_by[dc]
                remote(src.at[t], dst.at[me], s, (t,)).start()

    for c in range(0, 16, 4):
        to_rows(dot(pick, ffn_in[:, c * 128 : (c + 4) * 128]), c)
    pack(send1)
    arrived(blocks_of(1, 2), 0)
    arrived(blocks_of(1, 2), 1)
    quarter = half // 2
    push(wbuf.at[zz, y_by[3], :, pl.ds(0, quarter)], 26, in_y[0])
    push(wbuf.at[zz, y_by[1], :, pl.ds(quarter, quarter)], 26, in_y[1])
    push(wbuf.at[z_by[3], yy, :, pl.ds(half, quarter)], 27, in_z[0])
    push(wbuf.at[z_by[1], yy, :, pl.ds(half + quarter, quarter)], 27, in_z[1])

    with jax.named_scope("barrier_3"):
        pl.semaphore_wait(ready.at[1], len(in_group))

    second = {1: (8, 9), 2: (16, 17), 3: (18, 19)}
    third = {0: (10, 11), 1: (12, 13), 2: (20, 21), 3: (22, 23)}

    exchange(send1, arr1, 2, FAR_FIRST[:42])
    arr1[me] = send1[me]
    for to in in_z[:2]:
        push(wbuf.at[zz, y_by[1], :, left], second[1][0], to)
    for to in in_y[:2]:
        push(wbuf.at[z_by[1], yy, :, right], second[1][1], to)
    exchange(send1, arr1, 2, FAR_FIRST[42:85])
    for to in in_z[:2]:
        push(wbuf.at[zz, y_by[3], :, left], second[3][0], to)
    for to in in_y[:2]:
        push(wbuf.at[z_by[3], yy, :, right], second[3][1], to)
    exchange(send1, arr1, 2, FAR_FIRST[85:])
    arrived(blocks_of(1, 1), 26)
    arrived(blocks_of(1, 1), 27)
    for to in in_z[:2]:
        push(wbuf.at[zz, y_by[2], :, left], second[2][0], to)
    for to in in_y[:2]:
        push(wbuf.at[z_by[2], yy, :, right], second[2][1], to)
    for to in in_x:
        push(xg.at[xx, core], 3, to)

    arrived(blocks_of(1, 2), 4)
    arrived(blocks_of(1, 2), 5)
    push(wbuf.at[z_by[3], yy, :, left], 10, in_z[0])
    push(wbuf.at[zz, y_by[3], :, right], 11, in_y[0])
    def relay(d):
        arrived(blocks_of(1, 2), second[d][0])
        arrived(blocks_of(1, 2), second[d][1])
        side = 3 if d == 1 else 1
        push(wbuf.at[z_by[side], y_by[d], :, left], third[d][0], in_z[0 if side == 3 else 1])
        push(wbuf.at[z_by[d], y_by[side], :, right], third[d][1], in_y[0 if side == 3 else 1])

    relay(1)
    relay(3)

    for c in experts:
        c.wait()
    most = pl.ds(0, DEV - 1)
    arrived(arr1.at[most], 2)
    arrived(xg.at[pl.ds(0, 3), 0], 3)
    push(xg.at[:, core], 14, sibling)

    @pl.loop(0, DEV // 8)
    def _(i):
        for j in range(8):
            r = i * 8 + j
            tile32[pl.ds(pl.multiple_of(r * 16, 16), 16), :] = arr1[r].astype(F32)

    rows = jnp.concatenate([tile32[pl.ds(c, DEV, stride=16), :].astype(BF16) for c in range(16)], axis=1)
    hidden = (silu(dot(rows, eg[...])) * dot(rows, eu[...])).astype(BF16)
    for c in range(0, 16, 4):
        to_rows(dot(hidden, ed[:, c * 128 : (c + 4) * 128]), c)
    pack(send2)

    relay(2)
    for n in third[0]:
        arrived(blocks_of(1, 1), n)
    for n in third[1]:
        arrived(blocks_of(1, 1), n)
    exchange(send2, arr2, 6)
    arr2[me] = send2[me]

    arrived(xg.at[:, 0], 14)
    for n in third[2]:
        arrived(blocks_of(1, 1), n)
    for n in third[3]:
        arrived(blocks_of(1, 1), n)
    tokens = xg[...].reshape(GROUP * SEQ, D)

    def share(n):
        return wbuf[:, :, n * UNITS : (n + 1) * UNITS, :].reshape(RING * RING * UNITS, D)

    dense_hidden = (silu(nt_dot(tokens, share(0))) * nt_dot(tokens, share(1))).astype(BF16)
    for n, cols in enumerate((left, right)):
        part[:, :, :, cols] = dot(dense_hidden, share(2)[:, n * half : (n + 1) * half]).astype(BF16).reshape(RING, 2, SEQ, half)
        remote(part.at[:, 1 - core, :, cols], pair_in.at[:, :, cols], (15, 24)[n], sibling).start()
    for n, cols in enumerate((left, right)):
        arrived(pair_in.at[:, :, cols], (15, 24)[n])
        for x in range(RING):
            part2[x, :, cols] = (part[x, core, :, cols].astype(F32) + pair_in[x, :, cols].astype(F32)).astype(BF16)
        for d, to in zip((1, 3, 2), in_x):
            remote(part2.at[x_by[d], :, cols], parts_in.at[xx, :, cols], (7, 25)[n], to).start()
    parts_in[xx] = part2[xx]

    ffn_f = xg[xx, core].astype(F32)
    gate_value = jax.nn.sigmoid(jnp.sum(ffn_f * branch_gate[...], axis=-1, keepdims=True))
    arrived(arr2.at[most], 6)
    for t in range(SEQ):
        total = jnp.zeros((16, 128), F32)
        for k in range(TOP):
            total = total + route_weights[k, t] * arr2[routes[k, t]].astype(F32)
        tile32[pl.ds(t * 16, 16), :] = total
    for c in range(16):
        if c % 8 == 0:
            arrived(parts_in.at[pl.ds(0, RING - 1), :, (left, right)[c // 8]], (7, 25)[c // 8])
        cut = slice(c * 128, (c + 1) * 128)
        dense = parts_in[0, :, cut].astype(F32)
        for g in range(1, RING):
            dense = dense + parts_in[g, :, cut].astype(F32)
        out[:, cut] = (mid_s[:, cut] + tile32[pl.ds(c, SEQ, stride=16), :] + gate_value * dense).astype(BF16)

    results[0].start()

    with jax.named_scope("sent"):
        for n, many in enumerate(
            (
                blocks_of(1, 2),
                blocks_of(1, 2),
                send1.at[most],
                xg.at[pl.ds(0, 3), 0],
                blocks_of(1, 2),
                blocks_of(1, 2),
                send2.at[most],
                part2.at[pl.ds(0, 3), :, left],
                blocks_of(1, 2),
                blocks_of(1, 2),
                blocks_of(1, 1),
                blocks_of(1, 1),
                blocks_of(1, 1),
                blocks_of(1, 1),
                xg.at[:, 0],
                pair_in.at[:, :, left],
                blocks_of(1, 2),
                blocks_of(1, 2),
                blocks_of(1, 2),
                blocks_of(1, 2),
                blocks_of(1, 1),
                blocks_of(1, 1),
                blocks_of(1, 1),
                blocks_of(1, 1),
                pair_in.at[:, :, left],
                part2.at[pl.ds(0, 3), :, left],
                blocks_of(1, 1),
                blocks_of(1, 1),
            )
        ):
            waited(many, n)
        for c in results:
            c.wait()


def hand_on(*arrays):
    n = len(arrays)

    def body(*refs):
        ins, outs, held, sem = refs[:n], refs[n : 2 * n], refs[2 * n : 3 * n], refs[3 * n]
        gets = [pltpu.make_async_copy(ins[i], held[i], sem.at[i]) for i in range(n)]
        puts = [pltpu.make_async_copy(held[i], outs[i], sem.at[n + i]) for i in range(n)]
        for c in gets:
            c.start()
        for g, p in zip(gets, puts):
            g.wait()
            p.start()
        for c in puts:
            c.wait()

    spec = pl.BlockSpec(memory_space=pl.ANY)
    return pl.pallas_call(
        body,
        name="hand_on",
        out_shape=tuple(jax.ShapeDtypeStruct(a.shape, a.dtype) for a in arrays),
        in_specs=[spec] * n,
        out_specs=(spec,) * n,
        scratch_shapes=[pltpu.VMEM(a.shape, a.dtype) for a in arrays] + [pltpu.SemaphoreType.DMA((2 * n,))],
        compiler_params=pltpu.CompilerParams(vmem_limit_bytes=60 * 1024 * 1024),
    )(*arrays)


def per_device(
    hidden_in,
    lengths,
    attn_gain,
    query_weight,
    key_weight,
    value_weight,
    score_bias,
    out_weight,
    key_cache,
    value_cache,
    ffn_gain,
    routes,
    route_weights,
    expert_gate,
    expert_up,
    expert_down,
    dense_gate,
    dense_up,
    dense_down,
    branch_gate,
):
    hbm = pl.BlockSpec(memory_space=pl.ANY)
    dma = pltpu.SemaphoreType.DMA
    return hand_on(
        *pl.pallas_call(
            kernel,
            name="decode_layer",
            out_shape=(
                jax.ShapeDtypeStruct((SEQ, D), BF16),
                jax.ShapeDtypeStruct((SEQ, 128), BF16),
                jax.ShapeDtypeStruct((SEQ, 128), BF16),
            ),
            in_specs=[hbm] * 20,
            out_specs=(hbm, hbm, hbm),
            scratch_shapes=[
                pltpu.SMEM((SEQ,), jnp.int32),
                pltpu.SMEM((HEADS,), F32),
                pltpu.SMEM((TOP, SEQ), jnp.int32),
                pltpu.SMEM((TOP, SEQ), F32),
                pltpu.VMEM((SEQ, D), BF16),
                pltpu.VMEM((1, D), F32),
                pltpu.VMEM((1, D), F32),
                pltpu.VMEM((1, D), F32),
                pltpu.VMEM((TOP, SEQ), jnp.int32),
                pltpu.VMEM((SEQ, D), BF16),
                pltpu.VMEM((SEQ, 128), BF16),
                pltpu.VMEM((SEQ, 128), BF16),
                pltpu.VMEM((D, HEADS * HEAD), BF16),
                pltpu.VMEM((D, 128), BF16),
                pltpu.VMEM((D, 128), BF16),
                pltpu.VMEM((HEADS * HEAD, D), BF16),
                pltpu.VMEM((SEQ, LEN, 128), BF16),
                pltpu.VMEM((SEQ, LEN, 128), BF16),
                pltpu.VMEM((D, EFF), BF16),
                pltpu.VMEM((D, EFF), BF16),
                pltpu.VMEM((EFF, D), BF16),
                pltpu.VMEM((RING, RING, 3 * UNITS, D), BF16),
                pltpu.VMEM((RING, 2, SEQ, D), BF16),
                pltpu.VMEM((RING, 2, SEQ, D), BF16),
                pltpu.VMEM((RING, SEQ, D), BF16),
                pltpu.VMEM((RING, SEQ, D), BF16),
                pltpu.VMEM((RING, SEQ, D), BF16),
                pltpu.VMEM((DEV * 16, 128), F32),
                pltpu.VMEM((DEV, 16, 128), BF16),
                pltpu.VMEM((DEV, 16, 128), BF16),
                pltpu.VMEM((DEV, 16, 128), BF16),
                pltpu.VMEM((DEV, 16, 128), BF16),
                pltpu.VMEM((SEQ * HEADS, 128), F32),
                pltpu.VMEM((SEQ * HEADS, 128), F32),
                pltpu.VMEM((128, 256), BF16),
                pltpu.VMEM((SEQ, D), F32),
                dma((9,)),
                dma((3,)),
                dma((3 + HEADS,)),
                dma((SEQ,)),
                dma((SEQ,)),
                dma((3,)),
                dma((3,)),
                dma((28,)),
                dma((28,)),
                pltpu.SemaphoreType.REGULAR((2,)),
            ],
            compiler_params=pltpu.CompilerParams(
                collective_id=0, has_side_effects=True, vmem_limit_bytes=60 * 1024 * 1024
            ),
        )(
            lengths,
            score_bias,
            routes.T,
            route_weights.T,
            hidden_in,
            attn_gain.reshape(1, D),
            ffn_gain.reshape(1, D),
            branch_gate.reshape(1, D),
            query_weight,
            key_weight,
            value_weight,
            out_weight,
            key_cache,
            value_cache,
            expert_gate,
            expert_up,
            expert_down,
            dense_gate.T,
            dense_up.T,
            dense_down.T,
        )
    )


def solution(mesh):
    return jax.shard_map(
        per_device,
        mesh=mesh,
        in_specs=(
            P("ep", None),
            P("ep"),
            P(),
            P(),
            P(),
            P(),
            P(),
            P(),
            P("ep", None, None),
            P("ep", None, None),
            P(),
            P("ep", None),
            P("ep", None),
            P("ep", None, None),
            P("ep", None, None),
            P("ep", None, None),
            P(None, "ep"),
            P(None, "ep"),
            P(None, "ep"),
            P(),
        ),
        out_specs=(P("ep", None), P("ep", None), P("ep", None)),
        check_vma=False,
    )
```

```python
import itertools

import jax
import jax.numpy as jnp
from jax import lax
from jax.experimental import pallas as pl
from jax.experimental.pallas import tpu as pltpu
from jax.sharding import PartitionSpec as P

AXIS = "ep"
DEV = 128
GROUP = 8
RING = 4
SEQ = 16
D = 2048
LEN = 1024
HEAD = 64
HEADS = 8
TOP = 4
EFF = 512
UNITS = 16
EPS = 1e-06
MESH = pl.DeviceIdType.MESH
BF16 = jnp.bfloat16
FAR_FIRST = sorted(
    (o for o in itertools.product(range(RING), range(RING), range(RING), range(2)) if any(o)),
    key=lambda o: -sum(min(d, RING - d) for d in o[:3]),
)
F32 = jnp.float32


def rms_norm(values, gain):
    scale = lax.rsqrt(jnp.mean(values * values, axis=-1, keepdims=True) + EPS)
    return (values * scale * gain).astype(BF16)


def silu(v):
    return v / (1.0 + jnp.exp(-v))


def nt_dot(a, b):
    return lax.dot_general(a, b, (((1,), (1,)), ((), ())), preferred_element_type=F32)


def dot(a, b):
    return jnp.dot(a, b, preferred_element_type=F32)


def kernel(
    lens_h,
    bias_h,
    routes_h,
    route_weights_h,
    hid_h,
    attn_gain_h,
    ffn_gain_h,
    branch_gate_h,
    qw_h,
    kw_h,
    vw_h,
    ow_h,
    kc_h,
    vc_h,
    eg_h,
    eu_h,
    ed_h,
    dg_h,
    du_h,
    dd_h,
    out_h,
    new_keys_h,
    new_values_h,
    lens,
    bias,
    routes,
    route_weights,
    hid,
    attn_gain,
    ffn_gain,
    branch_gate,
    routes_v,
    out,
    new_keys,
    new_values,
    qw,
    kw,
    vw,
    ow,
    kc,
    vc,
    eg,
    eu,
    ed,
    wbuf,
    xg,
    part,
    part2,
    pair_in,
    parts_in,
    tile32,
    send1,
    arr1,
    send2,
    arr2,
    qs,
    os_,
    tri,
    mid_s,
    s_sem,
    o_sem,
    w_sem,
    k_sem,
    v_sem,
    e_sem,
    d_sem,
    snd,
    rcv,
    ready,
):
    me = lax.axis_index(AXIS)
    grp = me // GROUP
    mem = lax.rem(me, GROUP)
    zz = grp // RING
    yy = lax.rem(grp, RING)

    def device(z, y, member):
        return ((z * RING + y) * GROUP + member,)

    in_y = [device(zz, lax.rem(yy + d, RING), mem) for d in (1, 3, 2)]
    in_z = [device(lax.rem(zz + d, RING), yy, mem) for d in (1, 3, 2)]
    xx, core = mem // 2, lax.rem(mem, 2)
    in_x = [device(zz, yy, lax.rem(xx + d, RING) * 2 + core) for d in (1, 3, 2)]
    sibling = device(zz, yy, xx * 2 + 1 - core)
    in_group = [device(zz, yy, lax.rem(mem + d, GROUP)) for d in range(1, GROUP)]

    def signal(sem, devices):
        for to in devices:
            pl.semaphore_signal(sem, inc=1, device_id=to, device_id_type=MESH)

    barrier = pltpu.get_barrier_semaphore()
    signal(barrier, in_y + in_z + in_group)

    def copy(src, dst, sem):
        return pltpu.make_async_copy(src, dst, sem)

    own = [
        copy(dg_h, wbuf.at[zz, yy, pl.ds(0, UNITS)], d_sem.at[0]),
        copy(du_h, wbuf.at[zz, yy, pl.ds(UNITS, UNITS)], d_sem.at[1]),
        copy(dd_h, wbuf.at[zz, yy, pl.ds(2 * UNITS, UNITS)], d_sem.at[2]),
    ]
    proj = [copy(qw_h, qw, w_sem.at[0]), copy(kw_h, kw, w_sem.at[1]), copy(vw_h, vw, w_sem.at[2])]
    outw = [
        copy(
            ow_h.at[pl.ds(h * HEAD, HEAD)],
            ow.at[pl.ds((h % 4) * 2 * HEAD + (h // 4) * HEAD, HEAD)],
            w_sem.at[3 + h],
        )
        for h in range(HEADS)
    ]
    experts = [copy(eg_h.at[0], eg, e_sem.at[0]), copy(eu_h.at[0], eu, e_sem.at[1]), copy(ed_h.at[0], ed, e_sem.at[2])]
    first = [copy(hid_h, hid, s_sem.at[0]), copy(attn_gain_h, attn_gain, s_sem.at[1])]
    scalars = [copy(lens_h, lens, s_sem.at[2]), copy(bias_h, bias, s_sem.at[3])]
    later = [
        copy(ffn_gain_h, ffn_gain, s_sem.at[4]),
        copy(branch_gate_h, branch_gate, s_sem.at[5]),
        copy(routes_h, routes, s_sem.at[6]),
        copy(route_weights_h, route_weights, s_sem.at[7]),
        copy(routes_h, routes_v, s_sem.at[8]),
    ]
    results = [copy(out.at[:, pl.ds(n, D // 2)], out_h.at[:, pl.ds(n, D // 2)], o_sem.at[n * 2 // D]) for n in (0, D // 2)]
    results += [copy(new_keys, new_keys_h, o_sem.at[2]), copy(new_values, new_values_h, o_sem.at[3])]
    for c in own + first + proj + scalars:
        c.start()

    for first_b in (0, 8):

        @pl.loop(first_b, first_b + 8)
        def _(b):
            copy(kc_h.at[b], kc.at[b], k_sem.at[b]).start()

        @pl.loop(first_b, first_b + 8)
        def _(b):
            copy(vc_h.at[b], vc.at[b], v_sem.at[b]).start()

    for c in later + outw + experts:
        c.start()

    half = D // 2
    left, right = pl.ds(0, half), pl.ds(half, half)

    def remote(src, dst, s, to):
        return pltpu.make_async_remote_copy(
            src_ref=src, dst_ref=dst, send_sem=snd.at[s], recv_sem=rcv.at[s], device_id=to, device_id_type=MESH
        )

    def push(block, s, to):
        remote(block, block, s, to).start()

    def waited(ref, s):
        copy(ref, ref, snd.at[s]).wait()

    def arrived(ref, s):
        with jax.named_scope(f"arrived_{s}"):
            copy(ref, ref, rcv.at[s]).wait()

    def start_weights():
        with jax.named_scope("barrier_1"):
            pl.semaphore_wait(barrier, len(in_y + in_z + in_group))
        signal(ready.at[0], in_y)
        for c in own:
            c.wait()
        for to in in_y[:2]:
            push(wbuf.at[zz, yy, :, left], 0, to)
        for to in in_z[:2]:
            push(wbuf.at[zz, yy, :, right], 1, to)
        for to in in_z[:2]:
            push(wbuf.at[zz, yy, :, left], 4, to)
        for to in in_y[:2]:
            push(wbuf.at[zz, yy, :, right], 5, to)

    def blocks_of(a, b):
        return wbuf.at[pl.ds(0, a), pl.ds(0, b), :, left]

    x_by = [lax.rem(xx + d, RING) for d in range(RING)]
    core_by = [core, 1 - core]
    z_by = [lax.rem(zz + d, RING) for d in range(RING)]
    y_by = [lax.rem(yy + d, RING) for d in range(RING)]

    @pl.when(zz == 3)
    def _():
        start_weights()

    row = lax.broadcasted_iota(jnp.int32, (128, 256), 0)
    col = lax.broadcasted_iota(jnp.int32, (128, 256), 1)
    tri[...] = jnp.where((row > col) | (col >= 128), 1.0, 0.0).astype(BF16)

    for c in first:
        c.wait()
    normed = rms_norm(hid[...].astype(F32), attn_gain[...])
    for c in proj:
        c.wait()
    new_keys[...] = dot(normed, kw[...]).astype(BF16)
    new_values[...] = dot(normed, vw[...]).astype(BF16)
    for c in results[2:]:
        c.start()
    queries = dot(normed, qw[...]).astype(BF16).astype(F32)
    low = lax.broadcasted_iota(jnp.int32, (SEQ, 128), 1) < HEAD
    for h in range(HEADS):
        piece = queries[:, (h // 2) * 128 : (h // 2 + 1) * 128]
        if (h % 2) != (h // 4):
            piece = pltpu.roll(piece, HEAD, axis=1)
        piece = jnp.where(low, piece, 0.0) if h < 4 else jnp.where(low, 0.0, piece)
        qs[pl.ds(h, SEQ, stride=HEADS), :] = piece

    @pl.when((zz == 1) | (zz == 2))
    def _():
        start_weights()

    for c in scalars:
        c.wait()
    heads = lax.broadcasted_iota(jnp.int32, (HEADS, LEN), 0)
    bias_v = jnp.zeros((HEADS, LEN), F32)
    for h in range(HEADS):
        bias_v = jnp.where(heads == h, bias[h], bias_v)
    pos = lax.broadcasted_iota(jnp.int32, (HEADS, LEN), 1)
    blocks = LEN // 128

    @jax.named_scope("attend")
    def attend(start, count):
        logs, keeps, lives = [], [], []
        for b in range(start, start + count):
            copy(kc_h.at[b], kc.at[b], k_sem.at[b]).wait()
        for b in range(start, start + count):
            copy(vc_h.at[b], vc.at[b], v_sem.at[b]).wait()
        for j in range(count):
            b = start + j
            q = qs[pl.ds(b * HEADS, HEADS), :].astype(BF16)
            z = nt_dot(q, kc[b]) * (HEAD**-0.5) + bias_v
            live = pos < lens[b]
            t = jnp.log(1.0 + jnp.exp(-jnp.abs(z)))
            logs.append(jnp.minimum(z, 0.0) - t)
            keeps.append(jnp.where(live, jnp.minimum(-z, 0.0) - t, 0.0))
            lives.append(live)
        keep = jnp.concatenate(
            [keeps[j][:, c * 128 : (c + 1) * 128] for j in range(count) for c in range(blocks)], axis=0
        )
        hi = keep.astype(BF16)
        rest = keep - hi.astype(F32)
        mid = rest.astype(BF16)
        lo = (rest - mid.astype(F32)).astype(BF16)
        sums = dot(hi, tri[...]) + dot(mid, tri[...]) + dot(lo, tri[...])
        for j in range(count):
            b = start + j
            beyond = jnp.zeros((HEADS, 128), F32)
            pieces = [None] * blocks
            for c in reversed(range(blocks)):
                at = (j * blocks + c) * HEADS
                after = sums[at : at + HEADS, :128] + beyond
                beyond = beyond + sums[at : at + HEADS, 128:]
                cut = slice(c * 128, (c + 1) * 128)
                pieces[c] = jnp.where(lives[j][:, cut], jnp.exp(logs[j][:, cut] + after), 0.0)
            weights = jnp.concatenate(pieces, axis=1).astype(BF16)
            os_[pl.ds(b * HEADS, HEADS), :] = dot(weights, vc[b])

    attend(0, 8)

    @pl.when(zz == 0)
    def _():
        start_weights()

    attend(8, 8)
    with jax.named_scope("barrier_2"):
        pl.semaphore_wait(ready.at[0], len(in_y))
    signal(ready.at[1], in_group)

    for c in later + outw:
        c.wait()
    attended = []
    for h in range(4):
        first = os_[pl.ds(h, SEQ, stride=HEADS), :]
        second = os_[pl.ds(h + 4, SEQ, stride=HEADS), :]
        attended.append(jnp.where(low, first, second).astype(BF16))
    middle = hid[...].astype(F32) + dot(jnp.concatenate(attended, axis=1), ow[...])
    mid_s[...] = middle
    ffn_in = rms_norm(middle, ffn_gain[...])
    xg[xx, core] = ffn_in

    experts_i = lax.broadcasted_iota(jnp.int32, (DEV, SEQ), 0)
    hit = routes_v[0:1, :] == experts_i
    for k in range(1, TOP):
        hit = hit | (routes_v[k : k + 1, :] == experts_i)
    pick = jnp.where(hit, 1.0, 0.0).astype(BF16)

    def to_rows(values, c):
        for j in range(values.shape[1] // 128):
            tile32[pl.ds(c + j, DEV, stride=16), :] = values[:, j * 128 : (j + 1) * 128]

    def pack(dst):
        @pl.loop(0, DEV // 8)
        def _(i):
            for j in range(8):
                r = i * 8 + j
                dst[r] = tile32[pl.ds(pl.multiple_of(r * 16, 16), 16), :].astype(BF16)

    def exchange(src, dst, s, order=FAR_FIRST):
        with jax.named_scope(f"exchange_{s}"):

            for dz, dy, dx, dc in order:
                t = ((z_by[dz] * RING + y_by[dy]) * RING + x_by[dx]) * 2 + core_by[dc]
                remote(src.at[t], dst.at[me], s, (t,)).start()

    for c in range(0, 16, 4):
        to_rows(dot(pick, ffn_in[:, c * 128 : (c + 4) * 128]), c)
    pack(send1)
    arrived(blocks_of(1, 2), 0)
    arrived(blocks_of(1, 2), 1)
    quarter = half // 2
    push(wbuf.at[zz, y_by[3], :, pl.ds(0, quarter)], 26, in_y[0])
    push(wbuf.at[zz, y_by[1], :, pl.ds(quarter, quarter)], 26, in_y[1])
    push(wbuf.at[z_by[3], yy, :, pl.ds(half, quarter)], 27, in_z[0])
    push(wbuf.at[z_by[1], yy, :, pl.ds(half + quarter, quarter)], 27, in_z[1])

    with jax.named_scope("barrier_3"):
        pl.semaphore_wait(ready.at[1], len(in_group))

    second = {1: (8, 9), 2: (16, 17), 3: (18, 19)}
    third = {0: (10, 11), 1: (12, 13), 2: (20, 21), 3: (22, 23)}

    exchange(send1, arr1, 2, FAR_FIRST[:42])
    arr1[me] = send1[me]
    for to in in_z[:2]:
        push(wbuf.at[zz, y_by[1], :, left], second[1][0], to)
    for to in in_y[:2]:
        push(wbuf.at[z_by[1], yy, :, right], second[1][1], to)
    exchange(send1, arr1, 2, FAR_FIRST[42:85])
    for to in in_z[:2]:
        push(wbuf.at[zz, y_by[3], :, left], second[3][0], to)
    for to in in_y[:2]:
        push(wbuf.at[z_by[3], yy, :, right], second[3][1], to)
    exchange(send1, arr1, 2, FAR_FIRST[85:])
    arrived(blocks_of(1, 1), 26)
    arrived(blocks_of(1, 1), 27)
    for to in in_z[:2]:
        push(wbuf.at[zz, y_by[2], :, left], second[2][0], to)
    for to in in_y[:2]:
        push(wbuf.at[z_by[2], yy, :, right], second[2][1], to)
    for to in in_x:
        push(xg.at[xx, core], 3, to)

    arrived(blocks_of(1, 2), 4)
    arrived(blocks_of(1, 2), 5)
    push(wbuf.at[z_by[3], yy, :, left], 10, in_z[0])
    push(wbuf.at[zz, y_by[3], :, right], 11, in_y[0])
    def relay(d):
        arrived(blocks_of(1, 2), second[d][0])
        arrived(blocks_of(1, 2), second[d][1])
        side = 3 if d == 1 else 1
        push(wbuf.at[z_by[side], y_by[d], :, left], third[d][0], in_z[0 if side == 3 else 1])
        push(wbuf.at[z_by[d], y_by[side], :, right], third[d][1], in_y[0 if side == 3 else 1])

    relay(1)
    relay(3)

    for c in experts:
        c.wait()
    most = pl.ds(0, DEV - 1)
    arrived(arr1.at[most], 2)
    arrived(xg.at[pl.ds(0, 3), 0], 3)
    push(xg.at[:, core], 14, sibling)

    @pl.loop(0, DEV // 8)
    def _(i):
        for j in range(8):
            r = i * 8 + j
            tile32[pl.ds(pl.multiple_of(r * 16, 16), 16), :] = arr1[r].astype(F32)

    rows = jnp.concatenate([tile32[pl.ds(c, DEV, stride=16), :].astype(BF16) for c in range(16)], axis=1)
    hidden = (silu(dot(rows, eg[...])) * dot(rows, eu[...])).astype(BF16)
    for c in range(0, 16, 4):
        to_rows(dot(hidden, ed[:, c * 128 : (c + 4) * 128]), c)
    pack(send2)

    relay(2)
    for n in third[0]:
        arrived(blocks_of(1, 1), n)
    for n in third[1]:
        arrived(blocks_of(1, 1), n)
    exchange(send2, arr2, 6)
    arr2[me] = send2[me]

    arrived(xg.at[:, 0], 14)
    for n in third[2]:
        arrived(blocks_of(1, 1), n)
    for n in third[3]:
        arrived(blocks_of(1, 1), n)
    tokens = xg[...].reshape(GROUP * SEQ, D)

    def share(n):
        return wbuf[:, :, n * UNITS : (n + 1) * UNITS, :].reshape(RING * RING * UNITS, D)

    dense_hidden = (silu(nt_dot(tokens, share(0))) * nt_dot(tokens, share(1))).astype(BF16)
    for n, cols in enumerate((left, right)):
        part[:, :, :, cols] = dot(dense_hidden, share(2)[:, n * half : (n + 1) * half]).astype(BF16).reshape(RING, 2, SEQ, half)
        remote(part.at[:, 1 - core, :, cols], pair_in.at[:, :, cols], (15, 24)[n], sibling).start()
    for n, cols in enumerate((left, right)):
        arrived(pair_in.at[:, :, cols], (15, 24)[n])
        for x in range(RING):
            part2[x, :, cols] = (part[x, core, :, cols].astype(F32) + pair_in[x, :, cols].astype(F32)).astype(BF16)
        for d, to in zip((1, 3, 2), in_x):
            remote(part2.at[x_by[d], :, cols], parts_in.at[xx, :, cols], (7, 25)[n], to).start()
    parts_in[xx] = part2[xx]

    ffn_f = xg[xx, core].astype(F32)
    gate_value = jax.nn.sigmoid(jnp.sum(ffn_f * branch_gate[...], axis=-1, keepdims=True))
    arrived(arr2.at[most], 6)
    for t in range(SEQ):
        total = jnp.zeros((16, 128), F32)
        for k in range(TOP):
            total = total + route_weights[k, t] * arr2[routes[k, t]].astype(F32)
        tile32[pl.ds(t * 16, 16), :] = total
    for c in range(16):
        if c % 8 == 0:
            arrived(parts_in.at[pl.ds(0, RING - 1), :, (left, right)[c // 8]], (7, 25)[c // 8])
        cut = slice(c * 128, (c + 1) * 128)
        dense = parts_in[0, :, cut].astype(F32)
        for g in range(1, RING):
            dense = dense + parts_in[g, :, cut].astype(F32)
        out[:, cut] = (mid_s[:, cut] + tile32[pl.ds(c, SEQ, stride=16), :] + gate_value * dense).astype(BF16)
        if c % 8 == 7:
            results[c // 8].start()

    with jax.named_scope("sent"):
        for n, many in enumerate(
            (
                blocks_of(1, 2),
                blocks_of(1, 2),
                send1.at[most],
                xg.at[pl.ds(0, 3), 0],
                blocks_of(1, 2),
                blocks_of(1, 2),
                send2.at[most],
                part2.at[pl.ds(0, 3), :, left],
                blocks_of(1, 2),
                blocks_of(1, 2),
                blocks_of(1, 1),
                blocks_of(1, 1),
                blocks_of(1, 1),
                blocks_of(1, 1),
                xg.at[:, 0],
                pair_in.at[:, :, left],
                blocks_of(1, 2),
                blocks_of(1, 2),
                blocks_of(1, 2),
                blocks_of(1, 2),
                blocks_of(1, 1),
                blocks_of(1, 1),
                blocks_of(1, 1),
                blocks_of(1, 1),
                pair_in.at[:, :, left],
                part2.at[pl.ds(0, 3), :, left],
                blocks_of(1, 1),
                blocks_of(1, 1),
            )
        ):
            waited(many, n)
        for c in results:
            c.wait()


def hand_on(*arrays):
    n = len(arrays)

    def body(*refs):
        ins, outs, held, sem = refs[:n], refs[n : 2 * n], refs[2 * n : 3 * n], refs[3 * n]
        gets = [pltpu.make_async_copy(ins[i], held[i], sem.at[i]) for i in range(n)]
        puts = [pltpu.make_async_copy(held[i], outs[i], sem.at[n + i]) for i in range(n)]
        for c in gets:
            c.start()
        for g, p in zip(gets, puts):
            g.wait()
            p.start()
        for c in puts:
            c.wait()

    spec = pl.BlockSpec(memory_space=pl.ANY)
    return pl.pallas_call(
        body,
        name="hand_on",
        out_shape=tuple(jax.ShapeDtypeStruct(a.shape, a.dtype) for a in arrays),
        in_specs=[spec] * n,
        out_specs=(spec,) * n,
        scratch_shapes=[pltpu.VMEM(a.shape, a.dtype) for a in arrays] + [pltpu.SemaphoreType.DMA((2 * n,))],
        compiler_params=pltpu.CompilerParams(vmem_limit_bytes=60 * 1024 * 1024),
    )(*arrays)


def per_device(
    hidden_in,
    lengths,
    attn_gain,
    query_weight,
    key_weight,
    value_weight,
    score_bias,
    out_weight,
    key_cache,
    value_cache,
    ffn_gain,
    routes,
    route_weights,
    expert_gate,
    expert_up,
    expert_down,
    dense_gate,
    dense_up,
    dense_down,
    branch_gate,
):
    hbm = pl.BlockSpec(memory_space=pl.ANY)
    dma = pltpu.SemaphoreType.DMA
    return hand_on(
        *pl.pallas_call(
            kernel,
            name="decode_layer",
            out_shape=(
                jax.ShapeDtypeStruct((SEQ, D), BF16),
                jax.ShapeDtypeStruct((SEQ, 128), BF16),
                jax.ShapeDtypeStruct((SEQ, 128), BF16),
            ),
            in_specs=[hbm] * 20,
            out_specs=(hbm, hbm, hbm),
            scratch_shapes=[
                pltpu.SMEM((SEQ,), jnp.int32),
                pltpu.SMEM((HEADS,), F32),
                pltpu.SMEM((TOP, SEQ), jnp.int32),
                pltpu.SMEM((TOP, SEQ), F32),
                pltpu.VMEM((SEQ, D), BF16),
                pltpu.VMEM((1, D), F32),
                pltpu.VMEM((1, D), F32),
                pltpu.VMEM((1, D), F32),
                pltpu.VMEM((TOP, SEQ), jnp.int32),
                pltpu.VMEM((SEQ, D), BF16),
                pltpu.VMEM((SEQ, 128), BF16),
                pltpu.VMEM((SEQ, 128), BF16),
                pltpu.VMEM((D, HEADS * HEAD), BF16),
                pltpu.VMEM((D, 128), BF16),
                pltpu.VMEM((D, 128), BF16),
                pltpu.VMEM((HEADS * HEAD, D), BF16),
                pltpu.VMEM((SEQ, LEN, 128), BF16),
                pltpu.VMEM((SEQ, LEN, 128), BF16),
                pltpu.VMEM((D, EFF), BF16),
                pltpu.VMEM((D, EFF), BF16),
                pltpu.VMEM((EFF, D), BF16),
                pltpu.VMEM((RING, RING, 3 * UNITS, D), BF16),
                pltpu.VMEM((RING, 2, SEQ, D), BF16),
                pltpu.VMEM((RING, 2, SEQ, D), BF16),
                pltpu.VMEM((RING, SEQ, D), BF16),
                pltpu.VMEM((RING, SEQ, D), BF16),
                pltpu.VMEM((RING, SEQ, D), BF16),
                pltpu.VMEM((DEV * 16, 128), F32),
                pltpu.VMEM((DEV, 16, 128), BF16),
                pltpu.VMEM((DEV, 16, 128), BF16),
                pltpu.VMEM((DEV, 16, 128), BF16),
                pltpu.VMEM((DEV, 16, 128), BF16),
                pltpu.VMEM((SEQ * HEADS, 128), F32),
                pltpu.VMEM((SEQ * HEADS, 128), F32),
                pltpu.VMEM((128, 256), BF16),
                pltpu.VMEM((SEQ, D), F32),
                dma((9,)),
                dma((4,)),
                dma((3 + HEADS,)),
                dma((SEQ,)),
                dma((SEQ,)),
                dma((3,)),
                dma((3,)),
                dma((28,)),
                dma((28,)),
                pltpu.SemaphoreType.REGULAR((2,)),
            ],
            compiler_params=pltpu.CompilerParams(
                collective_id=0, has_side_effects=True, vmem_limit_bytes=60 * 1024 * 1024
            ),
        )(
            lengths,
            score_bias,
            routes.T,
            route_weights.T,
            hidden_in,
            attn_gain.reshape(1, D),
            ffn_gain.reshape(1, D),
            branch_gate.reshape(1, D),
            query_weight,
            key_weight,
            value_weight,
            out_weight,
            key_cache,
            value_cache,
            expert_gate,
            expert_up,
            expert_down,
            dense_gate.T,
            dense_up.T,
            dense_down.T,
        )
    )


def solution(mesh):
    return jax.shard_map(
        per_device,
        mesh=mesh,
        in_specs=(
            P("ep", None),
            P("ep"),
            P(),
            P(),
            P(),
            P(),
            P(),
            P(),
            P("ep", None, None),
            P("ep", None, None),
            P(),
            P("ep", None),
            P("ep", None),
            P("ep", None, None),
            P("ep", None, None),
            P("ep", None, None),
            P(None, "ep"),
            P(None, "ep"),
            P(None, "ep"),
            P(),
        ),
        out_specs=(P("ep", None), P("ep", None), P("ep", None)),
        check_vma=False,
    )
```
